1024 devices in a mesh: sp: 128 (over z, y), tp: 8 (over x, core).
Axes of the slice: x: 4, y: 8, z: 16, core: 2. Of those that a mesh axis runs over, the one named last changes fastest.
Arguments:
- tokens: bfloat16 [16384, 2048], P('sp', 'tp'), may hold values from -28 to 28
- norm_gain: bfloat16 [1, 2048], P(None, 'tp'), may hold values from 0.099609375 to 1.8984375
- conv_b_w: bfloat16 [2048, 1024], P(None, 'tp'), may hold values from -0.125 to 0.125
- conv_c_w: bfloat16 [2048, 1024], P(None, 'tp'), may hold values from -0.125 to 0.125
- conv_u_w: bfloat16 [2048, 1024], P(None, 'tp'), may hold values from -0.125 to 0.125
- conv_taps: bfloat16 [3, 1024], P(None, 'tp'), may hold values from -3.5 to 3.5
- query_w: bfloat16 [2048, 2048], P(None, 'tp'), may hold values from -0.125 to 0.125
- key_w: bfloat16 [2048, 2048], P(None, 'tp'), may hold values from -0.125 to 0.125
- value_w: bfloat16 [2048, 2048], P(None, 'tp'), may hold values from -0.125 to 0.125
- outgate_w: bfloat16 [2048, 2048], P(None, 'tp'), may hold values from -0.125 to 0.125
- gate_w: bfloat16 [2048, 2, 8], P(None, None, 'tp'), may hold values from -0.125 to 0.125
- gate_bias: float32 [2, 8], P(None, 'tp'), may hold values from -5 to 150
- mem_gain: bfloat16 [2048], P('tp'), may hold values from 0.099609375 to 1.8984375
- conv_out_w: bfloat16 [1024, 2048], P('tp'), may hold values from -0.1875 to 0.1875
- mem_out_w: bfloat16 [2048, 2048], P('tp'), may hold values from -0.125 to 0.125
Outputs:
- layer_out: bfloat16 [16384, 2048], P(('sp', 'tp'))
The draws below stay inside these ranges and needn't reach their ends.
All inputs are finite; a program needn't handle non-finite values.
Results may differ from the reference program's by a relative error of at most 0.014.
The reference program's roundings to bfloat16 on the way count: a program that leaves them out, or rounds other values in their place, can miss the bound.
Values may be sent and summed in bfloat16 or wider, within the bound.
No kernel may reach another device: no remote copies, remote signals or barrier semaphores. Data moves between devices by JAX's collectives and lax.ppermute only.
A program may use at most 64 MiB of HBM per device.

```python
import math
import jax
import jax.numpy as jnp
from jax import lax

D = 2048
CONV = 1024
MHEADS = 8
HEAD_DIM = 256
KW = 3
BLOCK = 128
MDIM = 2048
TOKENS = 16384
N_TP = 8


def draw_tokens(key, part):
    keys = jax.random.split(key, 3)
    row_scale = jnp.exp(jax.random.uniform(keys[0], (TOKENS, 1), jnp.float32, math.log(0.3), math.log(3.0)))
    col_scale = jnp.linspace(0.6, 1.8, D, dtype=jnp.float32)[None, :]
    col_scale = col_scale * jax.random.uniform(keys[1], (1, D), jnp.float32, 0.8, 1.25)
    base = jnp.clip(jax.random.normal(keys[2], (TOKENS, D), jnp.float32), -4.0, 4.0)
    return (base * row_scale * col_scale).astype(jnp.bfloat16)


def draw_gate_bias(key, part):
    keys = jax.random.split(key, 5)
    order = jax.random.permutation(keys[0], MHEADS)
    fast = order < MHEADS // 2
    input_part = -2.0 + 0.8 * jnp.clip(jax.random.normal(keys[2], (MHEADS,), jnp.float32), -3.0, 3.0)
    quick = jax.random.uniform(keys[3], (MHEADS,), jnp.float32, 3.0, 4.0)
    slow = jax.random.uniform(keys[4], (MHEADS,), jnp.float32, 10.5, 12.0)
    forget_part = jnp.where(fast, quick, slow)
    return jnp.stack([input_part, forget_part]).astype(jnp.float32)


def block_levels(key, shape, cuts, low, top_value):
    level, own = 1.0, jax.random.fold_in(key, 6)
    for dim, shards_of in cuts:
        steps = jnp.exp(jax.random.uniform(jax.random.fold_in(own, dim), (shards_of,), jnp.float32, low / len(cuts), top_value / len(cuts)))
        level = level * jnp.repeat(steps, shape[dim] // shards_of).reshape([-1 if axis == dim else 1 for axis in range(len(shape))])
    return level


def bell_draw(rng, extent, spread, most, shards=(), kind=jnp.bfloat16):
    level = block_levels(rng, extent, shards, -0.22, 0.18) if shards else 1.0
    values = jax.random.normal(rng, extent, jnp.float32) * spread * level
    return jnp.minimum(jnp.maximum(values, -most), most).astype(kind)


def setup_inputs(seed: int = 0) -> dict:
    arg_keys = jax.random.split(jax.random.key(seed), 16)
    tokens = draw_tokens(jax.random.fold_in(arg_keys[15], 71), 0)
    norm_gain = jnp.clip(1.0 + 0.18 * jax.random.normal(arg_keys[1], (1, D), jnp.float32), 0.099609375, 1.8984375).astype(jnp.bfloat16)
    conv_b_w = bell_draw(arg_keys[2], (D, CONV), D ** -0.5, 0.125, ((1, 8),))
    conv_c_w = bell_draw(arg_keys[3], (D, CONV), D ** -0.5, 0.125, ((1, 8),))
    conv_u_w = bell_draw(arg_keys[4], (D, CONV), D ** -0.5, 0.125, ((1, 8),))
    conv_taps = bell_draw(arg_keys[5], (KW, CONV), KW ** -0.5, 3.5, ((1, 8),))
    query_w = bell_draw(arg_keys[6], (D, MDIM), D ** -0.5, 0.125, ((1, 8),))
    key_w = bell_draw(arg_keys[7], (D, MDIM), D ** -0.5, 0.125, ((1, 8),))
    value_w = bell_draw(arg_keys[8], (D, MDIM), D ** -0.5, 0.125, ((1, 8),))
    outgate_w = bell_draw(arg_keys[9], (D, MDIM), D ** -0.5, 0.125, ((1, 8),))
    gate_w = bell_draw(arg_keys[10], (D, 2, MHEADS), D ** -0.5, 0.125, ((2, 8),))
    gate_bias = draw_gate_bias(jax.random.fold_in(arg_keys[15], 71), 0)
    mem_gain = jnp.clip(1.0 + 0.18 * jax.random.normal(arg_keys[12], (MDIM,), jnp.float32), 0.099609375, 1.8984375).astype(jnp.bfloat16)
    conv_out_w = bell_draw(arg_keys[13], (CONV, D), CONV ** -0.5, 0.1875, ((0, 8),))
    mem_out_w = bell_draw(arg_keys[14], (MDIM, D), MDIM ** -0.5, 0.125, ((0, 8),))
    return dict(tokens=tokens, norm_gain=norm_gain, conv_b_w=conv_b_w, conv_c_w=conv_c_w, conv_u_w=conv_u_w, conv_taps=conv_taps, query_w=query_w, key_w=key_w, value_w=value_w, outgate_w=outgate_w, gate_w=gate_w, gate_bias=gate_bias, mem_gain=mem_gain, conv_out_w=conv_out_w, mem_out_w=mem_out_w)


EPS = 1e-06
HIGH = lax.Precision.HIGHEST

def block_step(carry, inputs):
    memory, normer, stabil = carry
    query_block, key_block, value_block, input_gate, log_forget = inputs
    length = query_block.shape[0]
    causal = jnp.tril(jnp.ones((length, length), dtype=bool))
    running = jnp.cumsum(log_forget)
    decays = jnp.where(causal, running[:, None] - running[None, :] + input_gate[None, :], -jnp.inf)
    inter = running + stabil
    row_max = jnp.maximum(inter, lax.optimization_barrier(jnp.max(decays, axis=1)))
    weights = jnp.exp(decays - row_max[:, None])
    scores = jnp.dot(query_block, key_block.T, precision=HIGH) * weights
    carried = jnp.exp(inter - row_max)
    numer_part = carried[:, None] * jnp.dot(query_block, memory, precision=HIGH) + jnp.dot(scores, value_block, precision=HIGH)
    denom_part = carried * jnp.dot(query_block, normer, precision=HIGH) + lax.optimization_barrier(jnp.sum(scores, axis=1))
    result = numer_part / jnp.maximum(jnp.abs(denom_part), jnp.exp(-row_max))[:, None]
    new_stabil = row_max[-1]
    key_weight = jnp.exp(running[-1] - running + input_gate - new_stabil)
    fade = jnp.exp(running[-1] + stabil - new_stabil)
    memory = fade * memory + jnp.dot((key_weight[:, None] * key_block).T, value_block, precision=HIGH)
    normer = fade * normer + jnp.dot(key_weight, key_block, precision=HIGH)
    return ((memory, normer, new_stabil), result)

def memory_head(queries, keys, values, input_pre, log_forget):
    count, width = queries.shape
    blocks = count // BLOCK
    inputs = (queries.reshape(blocks, BLOCK, width), keys.reshape(blocks, BLOCK, width), values.reshape(blocks, BLOCK, width), input_pre.reshape(blocks, BLOCK), log_forget.reshape(blocks, BLOCK))
    start = (jnp.zeros((width, width), jnp.float32), jnp.zeros((width,), jnp.float32), jnp.zeros((), jnp.float32))
    final, results = lax.scan(block_step, start, inputs)
    return results.reshape(count, width)

def reference(tokens, norm_gain, conv_b_w, conv_c_w, conv_u_w, conv_taps, query_w, key_w, value_w, outgate_w, gate_w, gate_bias, mem_gain, conv_out_w, mem_out_w):
    wide = tokens.astype(jnp.float32)
    inv_rms = lax.rsqrt(lax.optimization_barrier(jnp.mean(wide * wide, axis=1, keepdims=True)) + EPS)
    scaled = (wide * norm_gain.astype(jnp.float32)).astype(jnp.bfloat16)

    def project(weight):
        rounded = (inv_rms * jnp.dot(scaled, weight, preferred_element_type=jnp.float32)).astype(jnp.bfloat16)
        return lax.optimization_barrier(rounded).astype(jnp.float32)
    gate_b = project(conv_b_w)
    gate_c = project(conv_c_w)
    gate_u = project(conv_u_w)
    queries = project(query_w)
    keys = project(key_w)
    values = project(value_w)
    outgate = project(outgate_w)
    gates = inv_rms * jnp.dot(scaled, gate_w.reshape(D, 2 * MHEADS), preferred_element_type=jnp.float32)
    input_pre = gates[:, :MHEADS] + gate_bias[0]
    forget_pre = gates[:, MHEADS:] + gate_bias[1]
    mixed_in = lax.optimization_barrier((gate_c * gate_u).astype(jnp.bfloat16)).astype(jnp.float32)
    padded = jnp.concatenate([jnp.zeros((KW - 1, CONV), jnp.float32), mixed_in], axis=0)
    taps = conv_taps.astype(jnp.float32)
    conv_sum = jnp.zeros((TOKENS, CONV), jnp.float32)
    for offset in range(KW):
        conv_sum = conv_sum + taps[offset] * padded[offset:offset + TOKENS]
    y_conv = (gate_b * conv_sum).astype(jnp.bfloat16)
    head_q = queries.reshape(TOKENS, MHEADS, HEAD_DIM)
    head_k = keys.reshape(TOKENS, MHEADS, HEAD_DIM) * HEAD_DIM ** (-0.5)
    head_v = values.reshape(TOKENS, MHEADS, HEAD_DIM)
    mem_raw = jax.vmap(memory_head, in_axes=1, out_axes=1)(head_q, head_k, head_v, input_pre, jax.nn.log_sigmoid(forget_pre))
    flat_raw = mem_raw.reshape(TOKENS, MDIM)
    mem_norm = flat_raw * lax.rsqrt(lax.optimization_barrier(jnp.mean(flat_raw * flat_raw, axis=1, keepdims=True)) + EPS)
    mem_norm = mem_norm * mem_gain.astype(jnp.float32)[None, :]
    y_mem = (jax.nn.sigmoid(outgate) * mem_norm).astype(jnp.bfloat16)
    conv_width = CONV // N_TP
    mem_width = MDIM // N_TP
    total = jnp.zeros((TOKENS, D), jnp.float32)
    for group in range(N_TP):
        part = jnp.dot(y_conv[:, group * conv_width:(group + 1) * conv_width], conv_out_w[group * conv_width:(group + 1) * conv_width], preferred_element_type=jnp.float32)
        part = part + jnp.dot(y_mem[:, group * mem_width:(group + 1) * mem_width], mem_out_w[group * mem_width:(group + 1) * mem_width], preferred_element_type=jnp.float32)
        total = total + lax.optimization_barrier(part.astype(jnp.bfloat16)).astype(jnp.float32)
    return total.astype(jnp.bfloat16)
```

```python
import functools

import jax
import jax.numpy as jnp
from jax import lax
from jax.experimental import pallas as pl
from jax.experimental.pallas import tpu as pltpu
from jax.sharding import Mesh
from jax.sharding import PartitionSpec as P

N = 128
HD = 256
MDIM = 2048
EPS = 1e-06
LOWEST = -1e30
ROWS = 80
TP = ("x", "c")
SP = ("z", "y")
BF = jnp.bfloat16
F32 = jnp.float32
INTERPRET = False


def call(kernel, outs, *args, name=None):
    return pl.pallas_call(
        kernel,
        out_shape=[jax.ShapeDtypeStruct(s, d) for s, d in outs],
        interpret=INTERPRET,
        name=name,
    )(*args)


def iota(dim):
    return lax.broadcasted_iota(jnp.int32, (N, N), dim)


def to_row(col):
    return jnp.sum(jnp.where(iota(0) == iota(1), col, 0.0), axis=0, keepdims=True)


def to_col(row):
    return jnp.sum(jnp.where(iota(0) == iota(1), row, 0.0), axis=1, keepdims=True)


def pieces(x):
    hi = x.astype(BF)
    rest = x - hi.astype(F32)
    mid = rest.astype(BF)
    low = (rest - mid.astype(F32)).astype(BF)
    return hi, mid, low


def dot(a, b):
    return jnp.dot(a, b, preferred_element_type=F32)


def dot_two(a, b):
    hi = a.astype(BF)
    return dot(hi, b) + dot((a - hi.astype(F32)).astype(BF), b)


def prepare(tok, gain, out):
    wide = tok[...].astype(F32)
    out[0, :N, :] = (wide * gain[...].astype(F32)).astype(BF)
    squares = to_row(jnp.sum(wide * wide, axis=1, keepdims=True))
    hi, mid, low = pieces(squares)
    zero = jnp.zeros((13, N), F32)
    tail = jnp.concatenate([hi.astype(F32), mid.astype(F32), low.astype(F32), zero], axis=0)
    out[0, N:, :N] = tail.astype(BF)
    out[0, N:, N:] = jnp.zeros((16, N), BF)


def log_sigmoid(x):
    e = jnp.exp(-jnp.abs(x))
    series = e * (1.0 - e * (0.5 - e * (1.0 / 3.0 - e * 0.25)))
    return -(jnp.maximum(-x, 0.0) + jnp.where(e < 0.01, series, jnp.log(1.0 + e)))


def states(tok, kw, vw, gw, bias, message, keys, values, aux):
    groups, _, part = tok.shape
    k_sum = jnp.zeros((N, HD), F32)
    v_sum = jnp.zeros((N, HD), F32)
    g_sum = jnp.zeros((N, 2), F32)
    sq = jnp.zeros((1, N), F32)
    for g in range(groups):
        piece = tok[g, :N, :]
        at = pl.ds(g * part, part)
        k_sum += dot(piece, kw[at, :])
        v_sum += dot(piece, vw[at, :])
        g_sum += dot(piece, gw[at, :])
        tail = tok[g, N:, :N].astype(F32)
        sq += tail[0:1] + tail[1:2] + tail[2:3]
    inv = lax.rsqrt(to_col(sq) / (groups * part) + EPS)
    k = (inv * k_sum).astype(BF)
    v = (inv * v_sum).astype(BF)
    keys[...] = k
    values[...] = v
    gates = inv * g_sum
    i_col = gates[:, 0:1] + bias[0:1, 0:1]
    lf_col = log_sigmoid(gates[:, 1:2] + bias[1:2, 0:1])
    lf_row = to_row(lf_col)
    i_row = to_row(i_col)
    lower = iota(1) <= iota(0)
    b_col = jnp.sum(jnp.where(lower, lf_row, 0.0), axis=1, keepdims=True)
    b_row = jnp.sum(jnp.where(iota(0) <= iota(1), lf_col, 0.0), axis=0, keepdims=True)
    b_all = jnp.sum(lf_col, axis=0, keepdims=True)
    after = jnp.sum(jnp.where(iota(1) > iota(0), lf_row, 0.0), axis=1, keepdims=True)
    weight = after + i_col
    top = jnp.max(weight, axis=0, keepdims=True)
    weight = jnp.exp(weight - top)
    kf = k.astype(F32) * HD**-0.5
    weighted = weight * kf
    hi = weighted.astype(BF)
    low = (weighted - hi.astype(F32)).astype(BF)
    across = (((0,), (0,)), ((), ()))
    memory = lax.dot_general(hi, v, across, preferred_element_type=F32)
    memory += lax.dot_general(low, v, across, preferred_element_type=F32)
    normer = jnp.sum(weighted, axis=0, keepdims=True)
    n_hi = normer.astype(BF).astype(F32)
    n_low = normer - n_hi
    lane = lambda a: jnp.broadcast_to(a, (1, N)).astype(F32)
    rest = [n_hi[:, :N], n_hi[:, N:], n_low[:, :N], n_low[:, N:]]
    rest += [lane(p) for p in pieces(b_all)] + [lane(p) for p in pieces(top)]
    rest = jnp.concatenate(rest + [jnp.zeros((16 - len(rest), N), F32)], axis=0).astype(BF)
    count, cut = message.shape[0], HD // message.shape[0]
    for y in range(count):
        rows = memory[y * cut : (y + 1) * cut].astype(BF)
        message[y, :cut, :] = rows[:, :N]
        message[y, cut : 2 * cut, :] = rows[:, N:]
        message[y, 2 * cut :, :] = rest
    aux[...] = jnp.concatenate([b_row, i_row, to_row(inv), jnp.zeros((5, N), F32)], axis=0)


def unpack(tail):
    t = tail.astype(F32)
    return t[0:2] + t[2:4], t[4:5] + t[5:6] + t[6:7], t[7:8] + t[8:9] + t[9:10]


def scales(sums, tops, upto):
    run, logs = jnp.zeros((1, N), F32), [None] * upto
    for j in reversed(range(upto)):
        logs[j] = tops[j] + run
        run = run + sums[j]
    return logs, run


def biggest(logs):
    top = jnp.full((1, N), LOWEST, F32)
    for a in logs:
        top = jnp.maximum(top, a)
    return top


def row_total(arrived, message):
    count, rows, _ = arrived.shape
    body = rows - 16
    extra = [unpack(arrived[j, body:, :]) for j in range(count)]
    logs, run = scales([e[1] for e in extra], [e[2] for e in extra], count)
    top = biggest(logs)
    total = jnp.zeros((body, N), F32)
    normer = jnp.zeros((2, N), F32)
    for j in range(count):
        w = jnp.exp(logs[j] - top)
        total += w * arrived[j, :body, :].astype(F32)
        normer += w * extra[j][0]
    n_hi = normer.astype(BF).astype(F32)
    rest = [n_hi, normer - n_hi] + [p.astype(F32) for p in pieces(run)]
    rest += [p.astype(F32) for p in pieces(top)] + [jnp.zeros((6, N), F32)]
    rest = jnp.concatenate(rest, axis=0).astype(BF)
    total = total.astype(BF)
    for z in range(message.shape[0]):
        message[z, :body, :] = total
        message[z, body:, :] = rest


def prefixes(place, row, column, message, own):
    z, y = place[0], place[1]
    count, rows, _ = row.shape
    body = rows - 16
    depth = column.shape[0]
    past = [unpack(column[j, body:, :]) for j in range(depth)]
    run, logs = jnp.zeros((1, N), F32), [None] * depth
    for j in reversed(range(depth)):
        logs[j] = jnp.where(j < z, past[j][2] + run, LOWEST)
        run = jnp.where(j < z, run + past[j][1], run)
    z_top = biggest(logs)
    before = jnp.zeros((body, N), F32)
    z_norm = jnp.zeros((2, N), F32)
    for j in range(depth):
        w = jnp.where(j < z, jnp.exp(logs[j] - z_top), 0.0)
        before += w * column[j, :body, :].astype(F32)
        z_norm += w * past[j][0]
    extra = [unpack(row[j, body:, :]) for j in range(count)]
    mine = jnp.zeros((3, N), F32)
    for t in range(count):
        logs, run = scales([e[1] for e in extra], [e[2] for e in extra], t)
        top = jnp.maximum(biggest(logs), z_top + run)
        w = jnp.exp(z_top + run - top)
        state = w * before
        norm = w * z_norm
        for j in range(t):
            w = jnp.exp(logs[j] - top)
            state += w * row[j, :body, :].astype(F32)
            norm += w * extra[j][0]
        message[t, :, :] = state.astype(BF)
        mine = jnp.where(t == y, jnp.concatenate([norm, top], axis=0), mine)
    own[...] = jnp.concatenate([mine, jnp.zeros((5, N), F32)], axis=0)


def inside(tok, aux, k_ref, v_ref, qw, ow, bw, cw, uw, gain, queries, numer, cols, gate, gate_b, mixed):
    groups, _, part = tok.shape
    sums = [jnp.zeros((N, w.shape[1]), F32) for w in (qw, ow, bw, cw, uw)]
    for g in range(groups):
        piece = tok[g, :N, :]
        at = pl.ds(g * part, part)
        sums = [s + dot(piece, w[at, :]) for s, w in zip(sums, (qw, ow, bw, cw, uw))]
    b_row, i_row = aux[0:1, :], aux[1:2, :]
    inv = to_col(aux[2:3, :])
    q, og, gb, gc, gu = [(inv * s).astype(BF) for s in sums]
    queries[...] = q
    gate_b[...] = gb
    mixed[...] = (gc.astype(F32) * gu.astype(F32)).astype(BF)
    gate[...] = jax.nn.sigmoid(og.astype(F32)) * gain[...].astype(F32)
    b_col = to_col(b_row)
    causal = iota(1) <= iota(0)
    decays = jnp.where(causal, b_col - b_row + i_row, LOWEST)
    top = jnp.max(decays, axis=1, keepdims=True)
    weights = jnp.where(causal, jnp.exp(decays - top), 0.0)
    scores = lax.dot_general(q, k_ref[...], (((1,), (1,)), ((), ())), preferred_element_type=F32)
    scores = scores * HD**-0.5 * weights
    numer[...] = dot_two(scores, v_ref[...])
    denom = jnp.sum(scores, axis=1, keepdims=True)
    lane = iota(1)
    cols[...] = jnp.where(lane == 0, b_col, jnp.where(lane == 1, top, jnp.where(lane == 2, denom, 0.0)))


def convolve(halo, mixed, gate_b, taps, weight, out):
    now = mixed[...].astype(F32)
    prev = halo[...].astype(F32)
    row = iota(0)
    one = jnp.where(row == 0, prev[1:2], pltpu.roll(now, 1, 0))
    two = jnp.where(row == 0, prev[0:1], jnp.where(row == 1, prev[1:2], pltpu.roll(now, 2, 0)))
    t = taps[...].astype(F32)
    total = t[0:1] * two + t[1:2] * one + t[2:3] * now
    y = (gate_b[...].astype(F32) * total).astype(BF)
    count, rows, _ = out.shape
    done = dot(y, weight[...]).astype(BF)
    for g in range(count):
        out[g, :, :] = done[g * rows : (g + 1) * rows]


def finish(arrived, own, queries, numer, cols, gate, weight, out):
    count, rows, _ = arrived.shape
    half = rows // 2
    q = queries[...]
    left = arrived[:, :half, :].reshape(HD, N)
    right = arrived[:, half:, :].reshape(HD, N)
    past = jnp.concatenate([dot(q, left), dot(q, right)], axis=1)
    qf = q.astype(F32)
    past_den = jnp.sum(qf[:, :N] * own[0:1, :] + qf[:, N:] * own[1:2, :], axis=1, keepdims=True)
    b_col, top, denom = cols[:, 0:1], cols[:, 1:2], cols[:, 2:3]
    inter = b_col + own[2:3, 0:1]
    most = jnp.maximum(inter, top)
    old, new = jnp.exp(inter - most), jnp.exp(top - most)
    den = old * past_den + new * denom
    raw = (old * past + new * numer[...]) / jnp.maximum(jnp.abs(den), jnp.exp(-most))
    squares = jnp.sum(raw * raw, axis=1, keepdims=True)
    y = (gate[...] * raw).astype(BF)
    done = dot(y, weight[...]).astype(BF)
    parts = [p.astype(F32) for p in pieces(squares)]
    lane = iota(1)
    tail = jnp.where(lane == 0, parts[0], jnp.where(lane == 1, parts[1], jnp.where(lane == 2, parts[2], 0.0)))
    tail = tail.astype(BF)
    groups, size, width = out.shape
    for g in range(groups):
        out[g, :, : width - N] = done[g * size : (g + 1) * size]
        out[g, :, width - N :] = tail[g * size : (g + 1) * size]


def gather_up(conv, mem, out):
    groups, _, width = conv.shape
    squares = jnp.zeros((conv.shape[1], 1), F32)
    for g in range(groups):
        tail = mem[g, :, width:].astype(F32)
        squares += tail[:, 0:1] + tail[:, 1:2] + tail[:, 2:3]
    scale = lax.rsqrt(squares / MDIM + EPS)
    c = jnp.zeros(conv.shape[1:], F32)
    m = jnp.zeros(conv.shape[1:], F32)
    for g in range(groups):
        c += conv[g].astype(F32)
        m += mem[g, :, :width].astype(F32)
    out[...] = (c + scale * m).astype(BF)


def exchange(value, axis):
    return lax.all_to_all(value, axis, split_axis=0, concat_axis=0, tiled=True)


def body(tokens, norm_gain, conv_b_w, conv_c_w, conv_u_w, conv_taps, query_w, key_w, value_w, outgate_w,
         gate_w, gate_bias, mem_gain, conv_out_w, mem_out_w):
    model = key_w.shape[0]
    nz, ny = lax.axis_size("z"), lax.axis_size("y")
    groups = lax.axis_size(TP)
    (local,) = call(prepare, [((1, N + 16, tokens.shape[1]), BF)], tokens, norm_gain, name="prepare")
    tok = lax.all_gather(local, TP, axis=0, tiled=True)
    slices = 2 * HD // ny
    message, keys, values, aux = call(
        states,
        [((ny, slices + 16, N), BF), ((N, HD), BF), ((N, HD), BF), ((8, N), F32)],
        tok, key_w, value_w, gate_w.reshape(model, 2), gate_bias, name="states",
    )
    row = exchange(message, "y")
    queries, numer, cols, gate, gate_b, mixed = call(
        inside,
        [((N, HD), BF), ((N, HD), F32), ((N, N), F32), ((N, HD), F32), ((N, N), BF), ((N, N), BF)],
        tok, aux, keys, values, query_w, outgate_w, conv_b_w, conv_c_w, conv_u_w, mem_gain[None, :], name="inside",
    )
    count = nz * ny
    halo = lax.ppermute(mixed[N - 2 :], SP, [(i, i + 1) for i in range(count - 1)])
    (total,) = call(row_total, [((nz, slices + 16, N), BF)], row, name="row_total")
    column = exchange(total, "z")
    (conv,) = call(convolve, [((groups, N // groups, model), BF)], halo, mixed, gate_b, conv_taps, conv_out_w, name="convolve")
    conv = exchange(conv, TP)
    place = jnp.stack([lax.axis_index("z"), lax.axis_index("y")]).astype(jnp.int32)
    back, own = pl.pallas_call(
        prefixes,
        out_shape=[jax.ShapeDtypeStruct((ny, slices, N), BF), jax.ShapeDtypeStruct((8, N), F32)],
        in_specs=[
            pl.BlockSpec(memory_space=pltpu.SMEM),
            pl.BlockSpec(memory_space=pltpu.VMEM),
            pl.BlockSpec(memory_space=pltpu.VMEM),
        ],
        interpret=INTERPRET,
        name="prefixes",
    )(place, row, column)
    state = exchange(back, "y")
    (mem,) = call(
        finish, [((groups, N // groups, model + N), BF)], state, own, queries, numer, cols, gate, mem_out_w, name="finish"
    )
    mem = exchange(mem, TP)
    (out,) = call(gather_up, [((N // groups, model), BF)], conv, mem, name="gather_up")
    return out


def solution(mesh):
    sp = mesh.shape["sp"]
    ny = 8 if sp % 8 == 0 else sp
    finer = Mesh(mesh.devices.reshape(sp // ny, ny, mesh.shape["tp"] // 2, 2), ("z", "y", "x", "c"))
    cols = P(None, TP)
    in_specs = (
        P(SP, TP), cols, cols, cols, cols, cols, cols, cols, cols, cols,
        P(None, None, TP), cols, P(TP), P(TP, None), P(TP, None),
    )
    return jax.shard_map(body, mesh=finer, in_specs=in_specs, out_specs=P(SP + TP, None), check_vma=False)
```

```python
import jax
import jax.numpy as jnp
from jax import lax
from jax.experimental import pallas as pl
from jax.experimental.pallas import tpu as pltpu
from jax.sharding import Mesh
from jax.sharding import PartitionSpec as P


N = 128
HD = 256
MDIM = 2048
EPS = 1e-06
LOWEST = -1e30
TP = "tp"
SP = "sp"
BF = jnp.bfloat16
F32 = jnp.float32
INTERPRET = False


def call(kernel, outs, *args, flops=0, scratch=(), specs=None, limit=16):
    options = {} if specs is None else {"in_specs": specs}
    return pl.pallas_call(
        kernel,
        out_shape=[jax.ShapeDtypeStruct(s, d) for s, d in outs],
        scratch_shapes=scratch,
        interpret=INTERPRET,
        compiler_params=pltpu.CompilerParams(vmem_limit_bytes=limit * 2**20),
        cost_estimate=pl.CostEstimate(flops=flops, bytes_accessed=flops // 1000, transcendentals=0) if flops else None,
        **options,
    )(*args)


def iota(dim):
    return lax.broadcasted_iota(jnp.int32, (N, N), dim)


def to_row(col):
    return jnp.sum(jnp.where(iota(0) == iota(1), col, 0.0), axis=0, keepdims=True)


def to_col(row):
    return jnp.sum(jnp.where(iota(0) == iota(1), row, 0.0), axis=1, keepdims=True)


def pieces(x):
    hi = x.astype(BF)
    rest = x - hi.astype(F32)
    mid = rest.astype(BF)
    low = (rest - mid.astype(F32)).astype(BF)
    return hi, mid, low


def dot(a, b):
    return jnp.dot(a, b, preferred_element_type=F32)


def dot_two(a, b):
    hi = a.astype(BF)
    return dot(hi, b) + dot((a - hi.astype(F32)).astype(BF), b)


def prepare(tok, gain, out):
    wide = tok[...].astype(F32)
    out[0, :N, :] = (wide * gain[...].astype(F32)).astype(BF)
    squares = to_row(jnp.sum(wide * wide, axis=1, keepdims=True))
    hi, mid, low = pieces(squares)
    zero = jnp.zeros((13, N), F32)
    tail = jnp.concatenate([hi.astype(F32), mid.astype(F32), low.astype(F32), zero], axis=0)
    out[0, N:, :N] = tail.astype(BF)
    out[0, N:, N:] = jnp.zeros((16, N), BF)


def log_sigmoid(x):
    e = jnp.exp(-jnp.abs(x))
    series = e * (1.0 - e * (0.5 - e * (1.0 / 3.0 - e * 0.25)))
    return -(jnp.maximum(-x, 0.0) + jnp.where(e < 0.01, series, jnp.log(1.0 + e)))


def states(tok, kw, vw, gw, bias, message, keys, values, aux, state):
    groups, _, part = tok.shape
    k_sum = jnp.zeros((N, HD), F32)
    v_sum = jnp.zeros((N, HD), F32)
    g_sum = jnp.zeros((N, 2), F32)
    sq = jnp.zeros((1, N), F32)
    for g in range(groups):
        piece = tok[g, :N, :]
        at = pl.ds(g * part, part)
        k_sum += dot(piece, kw[at, :])
        v_sum += dot(piece, vw[at, :])
        g_sum += lax.dot_general(piece, gw[:, at], (((1,), (1,)), ((), ())), preferred_element_type=F32)
        tail = tok[g, N:, :N].astype(F32)
        sq += tail[0:1] + tail[1:2] + tail[2:3]
    inv = lax.rsqrt(to_col(sq) / (groups * part) + EPS)
    k = (inv * k_sum).astype(BF)
    v = (inv * v_sum).astype(BF)
    keys[...] = k
    values[...] = v
    gates = inv * g_sum
    i_col = gates[:, 0:1] + bias[0:1, 0:1]
    lf_col = log_sigmoid(gates[:, 1:2] + bias[0:1, 1:2])
    lf_row = to_row(lf_col)
    i_row = to_row(i_col)
    lower = iota(1) <= iota(0)
    b_col = jnp.sum(jnp.where(lower, lf_row, 0.0), axis=1, keepdims=True)
    b_row = jnp.sum(jnp.where(iota(0) <= iota(1), lf_col, 0.0), axis=0, keepdims=True)
    b_all = jnp.sum(lf_col, axis=0, keepdims=True)
    after = jnp.sum(jnp.where(iota(1) > iota(0), lf_row, 0.0), axis=1, keepdims=True)
    weight = after + i_col
    top = jnp.max(weight, axis=0, keepdims=True)
    weight = jnp.exp(weight - top)
    kf = k.astype(F32) * HD**-0.5
    weighted = weight * kf
    hi = weighted.astype(BF)
    low = (weighted - hi.astype(F32)).astype(BF)
    across = (((0,), (0,)), ((), ()))
    memory = lax.dot_general(hi, v, across, preferred_element_type=F32)
    memory += lax.dot_general(low, v, across, preferred_element_type=F32)
    normer = jnp.sum(weighted, axis=0, keepdims=True)
    lane = lax.broadcasted_iota(jnp.int32, (1, N), 1)
    n_low = normer - normer.astype(BF).astype(F32)
    line = n_low[:, N:]
    for at, p in enumerate(pieces(b_all) + pieces(top)):
        line = jnp.where(lane == at, p.astype(F32), line)
    count, cut = message.shape[0], HD // message.shape[0]
    state[:, 0:cut, :] = memory[:, :N].reshape(count, cut, N)
    state[:, cut : 2 * cut, :] = memory[:, N:].reshape(count, cut, N)
    rest = jnp.concatenate([normer[:, :N], normer[:, N:], line, n_low[:, :N]], axis=0)
    state[:, 2 * cut :, :] = jnp.broadcast_to(rest[None], (count, 4, N))
    message[...] = state[...].astype(BF)
    aux[...] = jnp.concatenate([b_row, i_row, to_row(inv), jnp.zeros((5, N), F32)], axis=0)


def carry(place, arrived, message, own, state, back):
    count, rows, _ = arrived.shape
    slab = rows - 4
    state[...] = arrived[...].astype(F32)
    source = lax.broadcasted_iota(jnp.int32, (count, count), 1)
    target = lax.broadcasted_iota(jnp.int32, (count, count), 0)
    lines = state[:, slab + 2, :]
    tops = lines[:, 3:4] + lines[:, 4:5] + lines[:, 5:6]
    tops = jnp.sum(jnp.where(source == target, tops, 0.0), axis=0, keepdims=True)
    later = jnp.where(source < target, 1.0, 0.0)
    past = later.astype(BF)
    decay = jnp.zeros((count, count), F32)
    for p in range(3):
        decay += dot(past, (later * lines[:, p : p + 1]).astype(BF))
    logs = jnp.where(source < target, tops + decay, LOWEST)
    top = jnp.max(logs, axis=1, keepdims=True)
    weights = jnp.where(source < target, jnp.exp(logs - top), 0.0)
    hi = weights.astype(BF)
    low = (weights - hi.astype(F32)).astype(BF)
    mine = lax.broadcasted_iota(jnp.int32, (count, 1), 0) == place[0]
    pick = lambda a: jnp.sum(jnp.where(mine, a, 0.0), axis=0, keepdims=True)
    lines = []
    lane = lax.broadcasted_iota(jnp.int32, (1, N), 1)
    for r in range(rows):
        part = state[:, r, :]
        part = (jnp.where(lane < 6, 0.0, part) if r == slab + 2 else part).astype(BF)
        whole = dot(hi, part) + dot(low, part)
        if r < slab:
            back[:, r, :] = whole
        else:
            lines.append(pick(whole))
    message[...] = back[...].astype(BF)
    lines = [lines[0] + lines[3], lines[1] + lines[2], jnp.broadcast_to(pick(top), (1, N))]
    own[...] = jnp.concatenate(lines + [jnp.zeros((5, N), F32)], axis=0)


def inside(tok, aux, k_ref, v_ref, qw, ow, bw, cw, uw, gain, queries, numer, cols, gate, gate_b, mixed):
    groups, _, part = tok.shape
    sums = [jnp.zeros((N, w.shape[1]), F32) for w in (qw, ow, bw, cw, uw)]
    for g in range(groups):
        piece = tok[g, :N, :]
        at = pl.ds(g * part, part)
        sums = [s + dot(piece, w[at, :]) for s, w in zip(sums, (qw, ow, bw, cw, uw))]
    b_row, i_row = aux[0:1, :], aux[1:2, :]
    inv = to_col(aux[2:3, :])
    q, og, gb, gc, gu = [(inv * s).astype(BF) for s in sums]
    queries[...] = q
    gate_b[...] = gb
    mixed[...] = (gc.astype(F32) * gu.astype(F32)).astype(BF)
    gate[...] = jax.nn.sigmoid(og.astype(F32)) * gain[...].astype(F32).reshape(1, HD)
    b_col = to_col(b_row)
    causal = iota(1) <= iota(0)
    decays = jnp.where(causal, b_col - b_row + i_row, LOWEST)
    top = jnp.max(decays, axis=1, keepdims=True)
    weights = jnp.where(causal, jnp.exp(decays - top), 0.0)
    scores = lax.dot_general(q, k_ref[...], (((1,), (1,)), ((), ())), preferred_element_type=F32)
    scores = scores * HD**-0.5 * weights
    numer[...] = dot_two(scores, v_ref[...])
    denom = jnp.sum(scores, axis=1, keepdims=True)
    lane = iota(1)
    cols[...] = jnp.where(lane == 0, b_col, jnp.where(lane == 1, top, jnp.where(lane == 2, denom, 0.0)))


def convolve(halo, mixed, gate_b, taps, weight, out):
    now = mixed[...].astype(F32)
    prev = halo[...].astype(F32)
    row = iota(0)
    one = jnp.where(row == 0, prev[1:2], pltpu.roll(now, 1, 0))
    two = jnp.where(row == 0, prev[0:1], jnp.where(row == 1, prev[1:2], pltpu.roll(now, 2, 0)))
    t = taps[...].astype(F32)
    total = t[0:1] * two + t[1:2] * one + t[2:3] * now
    y = (gate_b[...].astype(F32) * total).astype(BF)
    count, rows, _ = out.shape
    done = dot(y, weight[...]).astype(BF)
    for g in range(count):
        out[g, :, :] = done[g * rows : (g + 1) * rows]


def finish(arrived, own, queries, numer, cols, gate, weight, out, state):
    _, rows, _ = arrived.shape
    half = rows // 2
    q = queries[...]
    state[...] = arrived[...].astype(F32)
    left = state[:, :half, :].reshape(HD, N).astype(BF)
    right = state[:, half:, :].reshape(HD, N).astype(BF)
    past = jnp.concatenate([dot(q, left), dot(q, right)], axis=1)
    qf = q.astype(F32)
    past_den = jnp.sum(qf[:, :N] * own[0:1, :] + qf[:, N:] * own[1:2, :], axis=1, keepdims=True)
    b_col, top, denom = cols[:, 0:1], cols[:, 1:2], cols[:, 2:3]
    inter = b_col + own[2:3, 0:1]
    most = jnp.maximum(inter, top)
    old, new = jnp.exp(inter - most), jnp.exp(top - most)
    den = old * past_den + new * denom
    raw = (old * past + new * numer[...]) / jnp.maximum(jnp.abs(den), jnp.exp(-most))
    squares = jnp.sum(raw * raw, axis=1, keepdims=True)
    y = (gate[...] * raw).astype(BF)
    done = dot(y, weight[...]).astype(BF)
    parts = [p.astype(F32) for p in pieces(squares)]
    lane = iota(1)
    tail = jnp.where(lane == 0, parts[0], jnp.where(lane == 1, parts[1], jnp.where(lane == 2, parts[2], 0.0)))
    tail = tail.astype(BF)
    groups, size, width = out.shape
    for g in range(groups):
        out[g, :, : width - N] = done[g * size : (g + 1) * size]
        out[g, :, width - N :] = tail[g * size : (g + 1) * size]


def gather_up(conv, mem, out):
    groups, _, width = conv.shape
    squares = jnp.zeros((conv.shape[1], 1), F32)
    for g in range(groups):
        tail = mem[g, :, width:].astype(F32)
        squares += tail[:, 0:1] + tail[:, 1:2] + tail[:, 2:3]
    scale = lax.rsqrt(squares / MDIM + EPS)
    c = jnp.zeros(conv.shape[1:], F32)
    m = jnp.zeros(conv.shape[1:], F32)
    for g in range(groups):
        c += conv[g].astype(F32)
        m += mem[g, :, :width].astype(F32)
    out[...] = (c + scale * m).astype(BF)


def exchange(value, axis):
    return lax.all_to_all(value, axis, split_axis=0, concat_axis=0, tiled=True)


def body(tokens, norm_gain, conv_b_w, conv_c_w, conv_u_w, conv_taps, query_w, key_w, value_w, outgate_w,
         gate_w, gate_bias, mem_gain, conv_out_w, mem_out_w):
    model = key_w.shape[0]
    count = lax.axis_size(SP)
    groups = lax.axis_size(TP)
    rows = 2 * HD // count
    (local,) = call(prepare, [((1, N + 16, tokens.shape[1]), BF)], tokens, norm_gain)
    tok = lax.all_gather(local, TP, axis=0, tiled=True)
    message, keys, values, aux = call(
        states,
        [((count, rows + 4, N), BF), ((N, HD), BF), ((N, HD), BF), ((8, N), F32)],
        tok, key_w, value_w, gate_w.reshape(model, 2).T, gate_bias.reshape(1, 2), flops=10**9,
        scratch=[pltpu.VMEM((count, rows + 4, N), F32)],
    )
    arrived = exchange(message, SP)
    queries, numer, cols, gate, gate_b, mixed = call(
        inside,
        [((N, HD), BF), ((N, HD), F32), ((N, N), F32), ((N, HD), F32), ((N, N), BF), ((N, N), BF)],
        tok, aux, keys, values, query_w, outgate_w, conv_b_w, conv_c_w, conv_u_w, mem_gain,
        flops=2 * 10**9,
    )
    halo = lax.ppermute(mixed[N - 2 :], SP, [(i, i + 1) for i in range(count - 1)])
    place = lax.axis_index(SP).reshape(1).astype(jnp.int32)
    vmem = pl.BlockSpec(memory_space=pltpu.VMEM)
    back, own = call(
        carry,
        [((count, rows, N), BF), ((8, N), F32)],
        place, arrived, flops=10**9,
        scratch=[pltpu.VMEM((count, rows + 4, N), F32), pltpu.VMEM((count, rows, N), F32)],
        specs=[pl.BlockSpec(memory_space=pltpu.SMEM), vmem],
    )
    state = exchange(back, SP)
    (conv,) = call(
        convolve, [((groups, N // groups, model), BF)], halo, mixed, gate_b, conv_taps, conv_out_w,
        flops=10**9,
    )
    conv = exchange(conv, TP)
    (mem,) = call(
        finish, [((groups, N // groups, model + N), BF)], state, own, queries, numer, cols, gate, mem_out_w,
        flops=10**9, scratch=[pltpu.VMEM((count, rows, N), F32)],
    )
    mem = exchange(mem, TP)
    (out,) = call(gather_up, [((N // groups, model), BF)], conv, mem)
    return out


def solution(mesh):
    sp = mesh.shape["sp"]
    finer = Mesh(mesh.devices.reshape(sp, mesh.shape["tp"]), ("sp", "tp"))
    cols = P(None, TP)
    in_specs = (
        P(SP, TP), cols, cols, cols, cols, cols, cols, cols, cols, cols,
        P(None, None, TP), cols, P(TP), P(TP, None), P(TP, None),
    )
    return jax.shard_map(body, mesh=finer, in_specs=in_specs, out_specs=P((SP, TP), None), check_vma=False)
```

```python
import jax
import jax.numpy as jnp
from jax import lax
from jax.experimental import pallas as pl
from jax.experimental.pallas import tpu as pltpu
from jax.sharding import Mesh
from jax.sharding import PartitionSpec as P


N = 128
HD = 256
MDIM = 2048
EPS = 1e-06
CHUNKS = 4
LOWEST = -1e30
TP = "tp"
SP = "sp"
BF = jnp.bfloat16
F32 = jnp.float32
INTERPRET = False


def call(kernel, outs, *args, flops=0, scratch=(), specs=None, limit=16):
    options = {} if specs is None else {"in_specs": specs}
    return pl.pallas_call(
        kernel,
        out_shape=[jax.ShapeDtypeStruct(s, d) for s, d in outs],
        scratch_shapes=scratch,
        interpret=INTERPRET,
        compiler_params=pltpu.CompilerParams(vmem_limit_bytes=limit * 2**20),
        cost_estimate=pl.CostEstimate(flops=flops, bytes_accessed=flops // 1000, transcendentals=0) if flops else None,
        **options,
    )(*args)


def iota(dim):
    return lax.broadcasted_iota(jnp.int32, (N, N), dim)


def to_row(col):
    return jnp.sum(jnp.where(iota(0) == iota(1), col, 0.0), axis=0, keepdims=True)


def to_col(row):
    return jnp.sum(jnp.where(iota(0) == iota(1), row, 0.0), axis=1, keepdims=True)


def pieces(x):
    hi = x.astype(BF)
    rest = x - hi.astype(F32)
    mid = rest.astype(BF)
    low = (rest - mid.astype(F32)).astype(BF)
    return hi, mid, low


def dot(a, b):
    return jnp.dot(a, b, preferred_element_type=F32)


def dot_two(a, b):
    hi = a.astype(BF)
    return dot(hi, b) + dot((a - hi.astype(F32)).astype(BF), b)


def fetched(pairs, sems):
    copies = [pltpu.make_async_copy(src, dst, sems.at[at]) for at, (src, dst) in enumerate(pairs)]
    for c in copies:
        c.start()
    return copies


def prepare(tok_hbm, gain_hbm, out, tok, gain, sems):
    for c in fetched([(tok_hbm, tok), (gain_hbm, gain)], sems):
        c.wait()
    wide = tok[...].astype(F32)
    out[0, :N, :] = (wide * gain[...].astype(F32)).astype(BF)
    squares = to_row(jnp.sum(wide * wide, axis=1, keepdims=True))
    hi, mid, low = pieces(squares)
    zero = jnp.zeros((13, N), F32)
    tail = jnp.concatenate([hi.astype(F32), mid.astype(F32), low.astype(F32), zero], axis=0)
    out[0, N:, :N] = tail.astype(BF)
    out[0, N:, N:] = jnp.zeros((16, N), BF)


def products(tok, sources, places, sems):
    groups, _, part = tok.shape
    step = groups * part // CHUNKS
    cut = [pl.ds(c * step, step) for c in range(CHUNKS)]
    copies = fetched([(s.at[at, :], p.at[at, :]) for at in cut for s, p in zip(sources, places)], sems)
    sums = [jnp.zeros((N, p.shape[1]), F32) for p in places]
    for c in range(CHUNKS):
        for each in copies[c * len(places) : (c + 1) * len(places)]:
            each.wait()
        for g in range(c * groups // CHUNKS, (c + 1) * groups // CHUNKS):
            piece = tok[g, :N, :]
            at = pl.ds(g * part, part)
            sums = [s + dot(piece, p[at, :]) for s, p in zip(sums, places)]
    return sums


def log_sigmoid(x):
    e = jnp.exp(-jnp.abs(x))
    series = e * (1.0 - e * (0.5 - e * (1.0 / 3.0 - e * 0.25)))
    return -(jnp.maximum(-x, 0.0) + jnp.where(e < 0.01, series, jnp.log(1.0 + e)))


def states(tok, kw_hbm, vw_hbm, gw, bias, message, kv, aux, state, kw, vw, sems):
    groups, _, part = tok.shape
    k_sum, v_sum = products(tok, (kw_hbm, vw_hbm), (kw, vw), sems)
    g_sum = jnp.zeros((N, 2), F32)
    sq = jnp.zeros((1, N), F32)
    for g in range(groups):
        at = pl.ds(g * part, part)
        g_sum += lax.dot_general(tok[g, :N, :], gw[:, at], (((1,), (1,)), ((), ())), preferred_element_type=F32)
        tail = tok[g, N:, :N].astype(F32)
        sq += tail[0:1] + tail[1:2] + tail[2:3]
    inv = lax.rsqrt(to_col(sq) / (groups * part) + EPS)
    k = (inv * k_sum).astype(BF)
    v = (inv * v_sum).astype(BF)
    kv[:, :HD] = k
    kv[:, HD:] = v
    gates = inv * g_sum
    i_col = gates[:, 0:1] + bias[0:1, 0:1]
    lf_col = log_sigmoid(gates[:, 1:2] + bias[0:1, 1:2])
    lf_row = to_row(lf_col)
    i_row = to_row(i_col)
    lower = iota(1) <= iota(0)
    b_col = jnp.sum(jnp.where(lower, lf_row, 0.0), axis=1, keepdims=True)
    b_row = jnp.sum(jnp.where(iota(0) <= iota(1), lf_col, 0.0), axis=0, keepdims=True)
    b_all = jnp.sum(lf_col, axis=0, keepdims=True)
    after = jnp.sum(jnp.where(iota(1) > iota(0), lf_row, 0.0), axis=1, keepdims=True)
    weight = after + i_col
    top = jnp.max(weight, axis=0, keepdims=True)
    weight = jnp.exp(weight - top)
    kf = k.astype(F32) * HD**-0.5
    weighted = weight * kf
    hi = weighted.astype(BF)
    low = (weighted - hi.astype(F32)).astype(BF)
    across = (((0,), (0,)), ((), ()))
    memory = lax.dot_general(hi, v, across, preferred_element_type=F32)
    memory += lax.dot_general(low, v, across, preferred_element_type=F32)
    normer = jnp.sum(weighted, axis=0, keepdims=True)
    lane = lax.broadcasted_iota(jnp.int32, (1, N), 1)
    n_low = normer - normer.astype(BF).astype(F32)
    line = n_low[:, N:]
    for at, p in enumerate(pieces(b_all) + pieces(top)):
        line = jnp.where(lane == at, p.astype(F32), line)
    count, cut = message.shape[0], HD // message.shape[0]
    state[:, 0:cut, :] = memory[:, :N].reshape(count, cut, N)
    state[:, cut : 2 * cut, :] = memory[:, N:].reshape(count, cut, N)
    rest = jnp.concatenate([normer[:, :N], normer[:, N:], line, n_low[:, :N]], axis=0)
    state[:, 2 * cut :, :] = jnp.broadcast_to(rest[None], (count, 4, N))
    message[...] = state[...].astype(BF)
    aux[...] = jnp.concatenate([b_row, i_row, to_row(inv), jnp.zeros((5, N), F32)], axis=0)


def carry(place, arrived, message, own, state, back):
    count, rows, _ = arrived.shape
    slab = rows - 4
    state[...] = arrived[...].astype(F32)
    source = lax.broadcasted_iota(jnp.int32, (count, count), 1)
    target = lax.broadcasted_iota(jnp.int32, (count, count), 0)
    lines = state[:, slab + 2, :]
    tops = lines[:, 3:4] + lines[:, 4:5] + lines[:, 5:6]
    tops = jnp.sum(jnp.where(source == target, tops, 0.0), axis=0, keepdims=True)
    later = jnp.where(source < target, 1.0, 0.0)
    past = later.astype(BF)
    decay = jnp.zeros((count, count), F32)
    for p in range(3):
        decay += dot(past, (later * lines[:, p : p + 1]).astype(BF))
    logs = jnp.where(source < target, tops + decay, LOWEST)
    top = jnp.max(logs, axis=1, keepdims=True)
    weights = jnp.where(source < target, jnp.exp(logs - top), 0.0)
    hi = weights.astype(BF)
    low = (weights - hi.astype(F32)).astype(BF)
    mine = lax.broadcasted_iota(jnp.int32, (count, 1), 0) == place[0]
    pick = lambda a: jnp.sum(jnp.where(mine, a, 0.0), axis=0, keepdims=True)
    lines = []
    lane = lax.broadcasted_iota(jnp.int32, (1, N), 1)
    for r in range(rows):
        part = state[:, r, :]
        part = (jnp.where(lane < 6, 0.0, part) if r == slab + 2 else part).astype(BF)
        whole = dot(hi, part) + dot(low, part)
        if r < slab:
            back[:, r, :] = whole
        else:
            lines.append(pick(whole))
    message[...] = back[...].astype(BF)
    lines = [lines[0] + lines[3], lines[1] + lines[2], jnp.broadcast_to(pick(top), (1, N))]
    own[...] = jnp.concatenate(lines + [jnp.zeros((5, N), F32)], axis=0)


def inside(tok, aux, kv, qw_hbm, ow_hbm, bw_hbm, cw_hbm, uw_hbm, gain, pack, gate_b, mixed, qw, ow, bw, cw, uw, sems):
    sums = products(tok, (qw_hbm, ow_hbm, bw_hbm, cw_hbm, uw_hbm), (qw, ow, bw, cw, uw), sems)
    b_row, i_row = aux[0:1, :], aux[1:2, :]
    inv = to_col(aux[2:3, :])
    q, og, gb, gc, gu = [(inv * s).astype(BF) for s in sums]
    pack[:, :HD] = q.astype(F32)
    gate_b[...] = gb
    mixed[...] = (gc.astype(F32) * gu.astype(F32)).astype(BF)
    pack[:, 2 * HD : 3 * HD] = jax.nn.sigmoid(og.astype(F32)) * gain[...].astype(F32).reshape(1, HD)
    b_col = to_col(b_row)
    causal = iota(1) <= iota(0)
    decays = jnp.where(causal, b_col - b_row + i_row, LOWEST)
    top = jnp.max(decays, axis=1, keepdims=True)
    weights = jnp.where(causal, jnp.exp(decays - top), 0.0)
    scores = lax.dot_general(q, kv[:, :HD], (((1,), (1,)), ((), ())), preferred_element_type=F32)
    scores = scores * HD**-0.5 * weights
    pack[:, HD : 2 * HD] = dot_two(scores, kv[:, HD:])
    denom = jnp.sum(scores, axis=1, keepdims=True)
    lane = iota(1)
    pack[:, 3 * HD :] = jnp.where(lane == 0, b_col, jnp.where(lane == 1, top, jnp.where(lane == 2, denom, 0.0)))


def convolve(halo, mixed, gate_b, taps, weight, out):
    now = mixed[...].astype(F32)
    prev = halo[...].astype(F32)
    row = iota(0)
    one = jnp.where(row == 0, prev[1:2], pltpu.roll(now, 1, 0))
    two = jnp.where(row == 0, prev[0:1], jnp.where(row == 1, prev[1:2], pltpu.roll(now, 2, 0)))
    t = taps[...].astype(F32)
    total = t[0:1] * two + t[1:2] * one + t[2:3] * now
    y = (gate_b[...].astype(F32) * total).astype(BF)
    out[...] = dot(y, weight[...]).astype(BF)


def finish(arrived, own, pack, conv, weight, out, state):
    _, rows, _ = arrived.shape
    half = rows // 2
    q = pack[:, :HD].astype(BF)
    state[...] = arrived[...].astype(F32)
    left = state[:, :half, :].reshape(HD, N).astype(BF)
    right = state[:, half:, :].reshape(HD, N).astype(BF)
    past = jnp.concatenate([dot(q, left), dot(q, right)], axis=1)
    past_den = jnp.sum(pack[:, :N] * own[0:1, :] + pack[:, N:HD] * own[1:2, :], axis=1, keepdims=True)
    cols = pack[:, 3 * HD :]
    b_col, top, denom = cols[:, 0:1], cols[:, 1:2], cols[:, 2:3]
    inter = b_col + own[2:3, 0:1]
    most = jnp.maximum(inter, top)
    old, new = jnp.exp(inter - most), jnp.exp(top - most)
    den = old * past_den + new * denom
    raw = (old * past + new * pack[:, HD : 2 * HD]) / jnp.maximum(jnp.abs(den), jnp.exp(-most))
    squares = jnp.sum(raw * raw, axis=1, keepdims=True)
    y = (pack[:, 2 * HD : 3 * HD] * raw).astype(BF)
    done = dot(y, weight[...]).astype(BF)
    parts = [p.astype(F32) for p in pieces(squares)]
    lane = iota(1)
    tail = jnp.where(lane == 0, parts[0], jnp.where(lane == 1, parts[1], jnp.where(lane == 2, parts[2], 0.0)))
    tail = tail.astype(BF)
    groups, size, _ = out.shape
    width = weight.shape[1]
    for g in range(groups):
        at = slice(g * size, (g + 1) * size)
        out[g, :, :width] = done[at]
        out[g, :, width : 2 * width] = conv[at]
        out[g, :, 2 * width :] = tail[at]


def gather_up(arrived, out):
    groups, size, width = arrived.shape
    width = (width - N) // 2
    squares = jnp.zeros((size, 1), F32)
    for g in range(groups):
        tail = arrived[g, :, 2 * width :].astype(F32)
        squares += tail[:, 0:1] + tail[:, 1:2] + tail[:, 2:3]
    scale = lax.rsqrt(squares / MDIM + EPS)
    c = jnp.zeros((size, width), F32)
    m = jnp.zeros((size, width), F32)
    for g in range(groups):
        m += arrived[g, :, :width].astype(F32)
        c += arrived[g, :, width : 2 * width].astype(F32)
    out[...] = (c + scale * m).astype(BF)


def exchange(value, axis):
    return lax.all_to_all(value, axis, split_axis=0, concat_axis=0, tiled=True)


def body(tokens, norm_gain, conv_b_w, conv_c_w, conv_u_w, conv_taps, query_w, key_w, value_w, outgate_w,
         gate_w, gate_bias, mem_gain, conv_out_w, mem_out_w):
    model = key_w.shape[0]
    count = lax.axis_size(SP)
    groups = lax.axis_size(TP)
    rows = 2 * HD // count
    vmem, hbm = pl.BlockSpec(memory_space=pltpu.VMEM), pl.BlockSpec(memory_space=pltpu.HBM)
    room = lambda *arrays: [pltpu.VMEM(a.shape, a.dtype) for a in arrays]
    sems = lambda n: [pltpu.SemaphoreType.DMA((n,))]
    (local,) = call(
        prepare, [((1, N + 16, tokens.shape[1]), BF)], tokens, norm_gain,
        specs=[hbm, hbm], scratch=room(tokens, norm_gain) + sems(2),
    )
    tok = lax.all_gather(local, TP, axis=0, tiled=True)
    message, kv, aux = call(
        states,
        [((count, rows + 4, N), BF), ((N, 2 * HD), BF), ((8, N), F32)],
        tok, key_w, value_w, gate_w.reshape(model, 2).T, gate_bias.reshape(1, 2), flops=10**9, limit=52,
        scratch=[pltpu.VMEM((count, rows + 4, N), F32)] + room(key_w, value_w) + sems(2 * CHUNKS),
        specs=[vmem, hbm, hbm, vmem, vmem],
    )
    arrived = exchange(message, SP)
    others = (query_w, outgate_w, conv_b_w, conv_c_w, conv_u_w)
    pack, gate_b, mixed = call(
        inside,
        [((N, 3 * HD + N), F32), ((N, N), BF), ((N, N), BF)],
        tok, aux, kv, *others, mem_gain, flops=2 * 10**9, limit=53,
        scratch=room(*others) + sems(5 * CHUNKS), specs=[vmem] * 3 + [hbm] * 5 + [vmem],
    )
    halo = lax.ppermute(mixed[N - 2 :], SP, [(i, i + 1) for i in range(count - 1)])
    (conv,) = call(convolve, [((N, model), BF)], halo, mixed, gate_b, conv_taps, conv_out_w, flops=10**9)
    place = lax.axis_index(SP).reshape(1).astype(jnp.int32)
    back, own = call(
        carry,
        [((count, rows, N), BF), ((8, N), F32)],
        place, arrived, flops=10**9,
        scratch=[pltpu.VMEM((count, rows + 4, N), F32), pltpu.VMEM((count, rows, N), F32)],
        specs=[pl.BlockSpec(memory_space=pltpu.SMEM), vmem],
    )
    state = exchange(back, SP)
    (mem,) = call(
        finish, [((groups, N // groups, 2 * model + N), BF)], state, own, pack, conv, mem_out_w,
        flops=10**9, scratch=[pltpu.VMEM((count, rows, N), F32)],
    )
    mem = exchange(mem, TP)
    (out,) = call(gather_up, [((N // groups, model), BF)], mem)
    return out


def solution(mesh):
    sp = mesh.shape["sp"]
    finer = Mesh(mesh.devices.reshape(sp, mesh.shape["tp"]), ("sp", "tp"))
    cols = P(None, TP)
    in_specs = (
        P(SP, TP), cols, cols, cols, cols, cols, cols, cols, cols, cols,
        P(None, None, TP), cols, P(TP), P(TP, None), P(TP, None),
    )
    return jax.shard_map(body, mesh=finer, in_specs=in_specs, out_specs=P((SP, TP), None), check_vma=False)
```

```python
import jax
import jax.numpy as jnp
from jax import lax
from jax.experimental import pallas as pl
from jax.experimental.pallas import tpu as pltpu
from jax.sharding import Mesh
from jax.sharding import PartitionSpec as P


N = 128
HD = 256
MDIM = 2048
EPS = 1e-06
OWN = 56
CHUNKS = 4
LOWEST = -1e30
TP = "tp"
SP = "sp"
BF = jnp.bfloat16
F32 = jnp.float32
INTERPRET = False


def call(kernel, outs, *args, flops=0, scratch=(), specs=None, limit=16):
    options = {} if specs is None else {"in_specs": specs}
    return pl.pallas_call(
        kernel,
        out_shape=[jax.ShapeDtypeStruct(s, d) for s, d in outs],
        scratch_shapes=scratch,
        interpret=INTERPRET,
        compiler_params=pltpu.CompilerParams(vmem_limit_bytes=limit * 2**20),
        cost_estimate=pl.CostEstimate(flops=flops, bytes_accessed=flops // 1000, transcendentals=0) if flops else None,
        **options,
    )(*args)


def iota(dim):
    return lax.broadcasted_iota(jnp.int32, (N, N), dim)


def to_row(col):
    return jnp.sum(jnp.where(iota(0) == iota(1), col, 0.0), axis=0, keepdims=True)


def to_col(row):
    return jnp.sum(jnp.where(iota(0) == iota(1), row, 0.0), axis=1, keepdims=True)


def pieces(x):
    hi = x.astype(BF)
    rest = x - hi.astype(F32)
    mid = rest.astype(BF)
    low = (rest - mid.astype(F32)).astype(BF)
    return hi, mid, low


def dot(a, b):
    return jnp.dot(a, b, preferred_element_type=F32)


def dot_two(a, b):
    hi = a.astype(BF)
    return dot(hi, b) + dot((a - hi.astype(F32)).astype(BF), b)


def fetched(pairs, sems):
    copies = [pltpu.make_async_copy(src, dst, sems.at[at]) for at, (src, dst) in enumerate(pairs)]
    for c in copies:
        c.start()
    return copies


def prepare(tok_hbm, gain_hbm, out, tok, gain, sems):
    for c in fetched([(tok_hbm, tok), (gain_hbm, gain)], sems):
        c.wait()
    wide = tok[...].astype(F32)
    out[0, :N, :] = (wide * gain[...].astype(F32)).astype(BF)
    squares = to_row(jnp.sum(wide * wide, axis=1, keepdims=True))
    hi, mid, low = pieces(squares)
    zero = jnp.zeros((13, N), F32)
    tail = jnp.concatenate([hi.astype(F32), mid.astype(F32), low.astype(F32), zero], axis=0)
    out[0, N:, :N] = tail.astype(BF)
    out[0, N:, N:] = jnp.zeros((16, N), BF)


def cuts(sources, places):
    step = places[0].shape[0] // CHUNKS
    cut = [pl.ds(c * step, step) for c in range(CHUNKS)]
    return [(s.at[at, :], p.at[at, :]) for at in cut for s, p in zip(sources, places)]


def products(tok, places, copies):
    groups, _, part = tok.shape
    sums = [jnp.zeros((N, p.shape[1]), F32) for p in places]
    for c in range(CHUNKS):
        for each in copies[c * len(places) : (c + 1) * len(places)]:
            each.wait()
        for g in range(c * groups // CHUNKS, (c + 1) * groups // CHUNKS):
            piece = tok[g, :N, :]
            at = pl.ds(g * part, part)
            sums = [s + dot(piece, p[at, :]) for s, p in zip(sums, places)]
    return sums


def log_sigmoid(x):
    e = jnp.exp(-jnp.abs(x))
    series = e * (1.0 - e * (0.5 - e * (1.0 / 3.0 - e * 0.25)))
    return -(jnp.maximum(-x, 0.0) + jnp.where(e < 0.01, series, jnp.log(1.0 + e)))


def states(tok_hbm, kw_hbm, vw_hbm, gw_hbm, bias_hbm, message, kv, aux, state, tok, kw, vw, gw, bias, first, sems):
    groups, _, part = tok.shape
    small = fetched([(tok_hbm, tok), (gw_hbm, gw), (bias_hbm, bias)], first)
    copies = fetched(cuts((kw_hbm, vw_hbm), (kw, vw)), sems)
    for c in small:
        c.wait()
    g_sum = jnp.zeros((N, 2), F32)
    sq = jnp.zeros((1, N), F32)
    for g in range(groups):
        at = pl.ds(g * part, part)
        g_sum += lax.dot_general(tok[g, :N, :], gw[:, at], (((1,), (1,)), ((), ())), preferred_element_type=F32)
        tail = tok[g, N:, :N].astype(F32)
        sq += tail[0:1] + tail[1:2] + tail[2:3]
    inv = lax.rsqrt(to_col(sq) / (groups * part) + EPS)
    gates = inv * g_sum
    i_col = gates[:, 0:1] + bias[0:1, 0:1]
    lf_col = log_sigmoid(gates[:, 1:2] + bias[0:1, 1:2])
    lf_row = to_row(lf_col)
    i_row = to_row(i_col)
    lower = iota(1) <= iota(0)
    b_col = jnp.sum(jnp.where(lower, lf_row, 0.0), axis=1, keepdims=True)
    b_row = jnp.sum(jnp.where(iota(0) <= iota(1), lf_col, 0.0), axis=0, keepdims=True)
    b_all = jnp.sum(lf_col, axis=0, keepdims=True)
    after = jnp.sum(jnp.where(iota(1) > iota(0), lf_row, 0.0), axis=1, keepdims=True)
    weight = after + i_col
    top = jnp.max(weight, axis=0, keepdims=True)
    weight = jnp.exp(weight - top)
    k_sum, v_sum = products(tok, (kw, vw), copies)
    k = (inv * k_sum).astype(BF)
    v = (inv * v_sum).astype(BF)
    kv[:, :HD] = k
    kv[:, HD:] = v
    kf = k.astype(F32) * HD**-0.5
    weighted = weight * kf
    hi = weighted.astype(BF)
    low = (weighted - hi.astype(F32)).astype(BF)
    across = (((0,), (0,)), ((), ()))
    memory = lax.dot_general(hi, v, across, preferred_element_type=F32)
    memory += lax.dot_general(low, v, across, preferred_element_type=F32)
    normer = jnp.sum(weighted, axis=0, keepdims=True)
    lane = lax.broadcasted_iota(jnp.int32, (1, N), 1)
    n_low = normer - normer.astype(BF).astype(F32)
    line = n_low[:, N:]
    for at, p in enumerate(pieces(b_all) + pieces(top)):
        line = jnp.where(lane == at, p.astype(F32), line)
    count, cut = message.shape[0], HD // message.shape[0]
    state[:, 0:cut, :] = memory[:, :N].reshape(count, cut, N)
    state[:, cut : 2 * cut, :] = memory[:, N:].reshape(count, cut, N)
    rest = jnp.concatenate([normer[:, :N], normer[:, N:], line, n_low[:, :N]], axis=0)
    state[:, 2 * cut :, :] = jnp.broadcast_to(rest[None], (count, 4, N))
    message[...] = state[...].astype(BF)
    aux[...] = jnp.concatenate([b_row, i_row, to_row(inv), jnp.zeros((5, N), F32)], axis=0)


def carry(place, arrived, message, own, state, back):
    count, rows, _ = arrived.shape
    slab = rows - 4
    state[...] = arrived[...].astype(F32)
    source = lax.broadcasted_iota(jnp.int32, (count, count), 1)
    target = lax.broadcasted_iota(jnp.int32, (count, count), 0)
    lines = state[:, slab + 2, :]
    tops = lines[:, 3:4] + lines[:, 4:5] + lines[:, 5:6]
    tops = jnp.sum(jnp.where(source == target, tops, 0.0), axis=0, keepdims=True)
    later = jnp.where(source < target, 1.0, 0.0)
    past = later.astype(BF)
    decay = jnp.zeros((count, count), F32)
    for p in range(3):
        decay += dot(past, (later * lines[:, p : p + 1]).astype(BF))
    logs = jnp.where(source < target, tops + decay, LOWEST)
    top = jnp.max(logs, axis=1, keepdims=True)
    weights = jnp.where(source < target, jnp.exp(logs - top), 0.0)
    hi = weights.astype(BF)
    low = (weights - hi.astype(F32)).astype(BF)
    mine = lax.broadcasted_iota(jnp.int32, (count, 1), 0) == place[0]
    pick = lambda a: jnp.sum(jnp.where(mine, a, 0.0), axis=0, keepdims=True)
    lines = []
    lane = lax.broadcasted_iota(jnp.int32, (1, N), 1)
    for r in range(rows):
        part = state[:, r, :]
        part = (jnp.where(lane < 6, 0.0, part) if r == slab + 2 else part).astype(BF)
        whole = dot(hi, part) + dot(low, part)
        if r < slab:
            back[:, r, :] = whole
        else:
            lines.append(pick(whole))
    message[...] = back[...].astype(BF)
    lines = [lines[0] + lines[3], lines[1] + lines[2], jnp.broadcast_to(pick(top), (1, N))]
    own[...] = jnp.concatenate(lines + [jnp.zeros((5, N), F32)], axis=0)


def mixing(tok_hbm, aux_hbm, bw_hbm, cw_hbm, uw_hbm, gate_b, mixed, tok, aux, bw, cw, uw, first, sems):
    small = fetched([(tok_hbm, tok), (aux_hbm, aux)], first)
    copies = fetched(cuts((bw_hbm, cw_hbm, uw_hbm), (bw, cw, uw)), sems)
    for c in small:
        c.wait()
    inv = to_col(aux[2:3, :])
    gb, gc, gu = [(inv * s).astype(BF) for s in products(tok, (bw, cw, uw), copies)]
    gate_b[...] = gb
    mixed[...] = (gc.astype(F32) * gu.astype(F32)).astype(BF)


def inside(tok_hbm, aux_hbm, kv_hbm, qw_hbm, ow_hbm, gain_hbm, pack, tok, aux, kv, qw, ow, gain, first, sems):
    small = fetched([(tok_hbm, tok), (aux_hbm, aux), (kv_hbm, kv), (gain_hbm, gain)], first)
    copies = fetched(cuts((qw_hbm, ow_hbm), (qw, ow)), sems)
    for c in small:
        c.wait()
    b_row, i_row = aux[0:1, :], aux[1:2, :]
    inv = to_col(aux[2:3, :])
    q, og = [(inv * s).astype(BF) for s in products(tok, (qw, ow), copies)]
    pack[:, :HD] = q.astype(F32)
    pack[:, 2 * HD : 3 * HD] = jax.nn.sigmoid(og.astype(F32)) * gain[...].astype(F32).reshape(1, HD)
    b_col = to_col(b_row)
    causal = iota(1) <= iota(0)
    decays = jnp.where(causal, b_col - b_row + i_row, LOWEST)
    top = jnp.max(decays, axis=1, keepdims=True)
    weights = jnp.where(causal, jnp.exp(decays - top), 0.0)
    scores = lax.dot_general(q, kv[:, :HD], (((1,), (1,)), ((), ())), preferred_element_type=F32)
    scores = scores * HD**-0.5 * weights
    pack[:, HD : 2 * HD] = dot_two(scores, kv[:, HD:])
    denom = jnp.sum(scores, axis=1, keepdims=True)
    lane = iota(1)
    pack[:, 3 * HD :] = jnp.where(lane == 0, b_col, jnp.where(lane == 1, top, jnp.where(lane == 2, denom, 0.0)))


def convolve(place, halo, mixed, gate_b, taps, weight, keep, send):
    now = mixed[...].astype(F32)
    prev = halo[...].astype(F32)
    row = iota(0)
    one = jnp.where(row == 0, prev[1:2], pltpu.roll(now, 1, 0))
    two = jnp.where(row == 0, prev[0:1], jnp.where(row == 1, prev[1:2], pltpu.roll(now, 2, 0)))
    t = taps[...].astype(F32)
    total = t[0:1] * two + t[1:2] * one + t[2:3] * now
    y = (gate_b[...].astype(F32) * total).astype(BF)
    done = dot(y, weight[...]).astype(BF)
    half = done.shape[1] // 2
    left, right = done[:, :half], done[:, half:]
    first = place[0] % 2 == 0
    keep[...] = jnp.where(first, left, right)
    send[...] = jnp.where(first, right, left)


def finish(arrived, own, pack, keep, other, weight, out, state):
    _, rows, _ = arrived.shape
    half = rows // 2
    q = pack[:, :HD].astype(BF)
    state[...] = arrived[...].astype(F32)
    left = state[:, :half, :].reshape(HD, N).astype(BF)
    right = state[:, half:, :].reshape(HD, N).astype(BF)
    past = jnp.concatenate([dot(q, left), dot(q, right)], axis=1)
    past_den = jnp.sum(pack[:, :N] * own[0:1, :] + pack[:, N:HD] * own[1:2, :], axis=1, keepdims=True)
    cols = pack[:, 3 * HD :]
    b_col, top, denom = cols[:, 0:1], cols[:, 1:2], cols[:, 2:3]
    inter = b_col + own[2:3, 0:1]
    most = jnp.maximum(inter, top)
    old, new = jnp.exp(inter - most), jnp.exp(top - most)
    den = old * past_den + new * denom
    raw = (old * past + new * pack[:, HD : 2 * HD]) / jnp.maximum(jnp.abs(den), jnp.exp(-most))
    squares = jnp.sum(raw * raw, axis=1, keepdims=True)
    y = (pack[:, 2 * HD : 3 * HD] * raw).astype(BF)
    done = dot(y, weight[...]).astype(BF)
    parts = [p.astype(F32) for p in pieces(squares)]
    lane = iota(1)
    tail = jnp.where(lane == 0, parts[0], jnp.where(lane == 1, parts[1], jnp.where(lane == 2, parts[2], 0.0)))
    tail = tail.astype(BF)
    groups, size, _ = out.shape
    width = weight.shape[1]
    conv = (keep[...].astype(F32) + other[...].astype(F32)).astype(BF)
    for g in range(groups):
        at = slice(g * size, (g + 1) * size)
        out[g, :, :width] = done[at]
        out[g, :, width : width + width // 2] = conv[at]
        out[g, :, width + width // 2 :] = tail[at]


def gather_up(arrived, out):
    groups, size, width = arrived.shape
    half = (width - N) // 3
    squares = jnp.zeros((size, 1), F32)
    for g in range(groups):
        tail = arrived[g, :, 3 * half :].astype(F32)
        squares += tail[:, 0:1] + tail[:, 1:2] + tail[:, 2:3]
    scale = lax.rsqrt(squares / MDIM + EPS)
    for side in range(2):
        at = slice(side * half, (side + 1) * half)
        m = jnp.zeros((size, half), F32)
        c = jnp.zeros((size, half), F32)
        for g in range(groups):
            m += arrived[g, :, at].astype(F32)
        for g in range(side, groups, 2):
            c += arrived[g, :, 2 * half : 3 * half].astype(F32)
        out[:, at] = (c + scale * m).astype(BF)


def exchange(value, axis):
    return lax.all_to_all(value, axis, split_axis=0, concat_axis=0, tiled=True)


def body(tokens, norm_gain, conv_b_w, conv_c_w, conv_u_w, conv_taps, query_w, key_w, value_w, outgate_w,
         gate_w, gate_bias, mem_gain, conv_out_w, mem_out_w):
    model = key_w.shape[0]
    count = lax.axis_size(SP)
    groups = lax.axis_size(TP)
    rows = 2 * HD // count
    vmem, hbm = pl.BlockSpec(memory_space=pltpu.VMEM), pl.BlockSpec(memory_space=pltpu.HBM)
    room = lambda *arrays: [pltpu.VMEM(a.shape, a.dtype) for a in arrays]
    sems = lambda n: [pltpu.SemaphoreType.DMA((n,))]
    vmem, hbm, smem = [pl.BlockSpec(memory_space=m) for m in (pltpu.VMEM, pltpu.HBM, pltpu.SMEM)]
    room = lambda *arrays: [pltpu.VMEM(a.shape, a.dtype) for a in arrays]
    sems = lambda *ns: [pltpu.SemaphoreType.DMA((n,)) for n in ns]
    (local,) = call(
        prepare, [((1, N + 16, tokens.shape[1]), BF)], tokens, norm_gain,
        specs=[hbm] * 2, scratch=room(tokens, norm_gain) + sems(2), limit=OWN,
    )
    tok = lax.all_gather(local, TP, axis=0, tiled=True)
    taken = (tok, key_w, value_w, gate_w.reshape(model, 2).T, gate_bias.reshape(1, 2))
    message, kv, aux = call(
        states,
        [((count, rows + 4, N), BF), ((N, 2 * HD), BF), ((8, N), F32)],
        *taken, flops=10**9, specs=[hbm] * 5, limit=OWN,
        scratch=[pltpu.VMEM((count, rows + 4, N), F32)] + room(*taken) + sems(3, 2 * CHUNKS),
    )
    arrived = exchange(message, SP)
    taken = (tok, aux, conv_b_w, conv_c_w, conv_u_w)
    gate_b, mixed = call(
        mixing, [((N, N), BF), ((N, N), BF)], *taken, flops=10**9, specs=[hbm] * 5, limit=OWN,
        scratch=room(*taken) + sems(2, 3 * CHUNKS),
    )
    halo = lax.ppermute(mixed[N - 2 :], SP, [(i, i + 1) for i in range(count - 1)])
    taken = (tok, aux, kv, query_w, outgate_w, mem_gain)
    (pack,) = call(
        inside, [((N, 3 * HD + N), F32)], *taken, flops=10**9, specs=[hbm] * 6, limit=OWN,
        scratch=room(*taken) + sems(4, 2 * CHUNKS),
    )
    core = lax.axis_index(TP).reshape(1).astype(jnp.int32)
    keep, send = call(
        convolve, [((N, model // 2), BF), ((N, model // 2), BF)], core, halo, mixed, gate_b, conv_taps, conv_out_w,
        flops=10**9, specs=[smem] + [vmem] * 5,
    )
    other = lax.ppermute(send, TP, [(i, i ^ 1) for i in range(groups)])
    place = lax.axis_index(SP).reshape(1).astype(jnp.int32)
    back, own = call(
        carry,
        [((count, rows, N), BF), ((8, N), F32)],
        place, arrived, flops=10**9,
        scratch=[pltpu.VMEM((count, rows + 4, N), F32), pltpu.VMEM((count, rows, N), F32)],
        specs=[smem, vmem],
    )
    state = exchange(back, SP)
    (mem,) = call(
        finish, [((groups, N // groups, 3 * model // 2 + N), BF)], state, own, pack, keep, other, mem_out_w,
        flops=10**9, scratch=[pltpu.VMEM((count, rows, N), F32)],
    )
    mem = exchange(mem, TP)
    (out,) = call(gather_up, [((N // groups, model), BF)], mem)
    return out


def solution(mesh):
    sp = mesh.shape["sp"]
    finer = Mesh(mesh.devices.reshape(sp, mesh.shape["tp"]), ("sp", "tp"))
    cols = P(None, TP)
    in_specs = (
        P(SP, TP), cols, cols, cols, cols, cols, cols, cols, cols, cols,
        P(None, None, TP), cols, P(TP), P(TP, None), P(TP, None),
    )
    return jax.shard_map(body, mesh=finer, in_specs=in_specs, out_specs=P((SP, TP), None), check_vma=False)
```

```python
import jax
import jax.numpy as jnp
from jax import lax
from jax.experimental import pallas as pl
from jax.experimental.pallas import tpu as pltpu
from jax.sharding import Mesh
from jax.sharding import PartitionSpec as P


N = 128
HD = 256
MDIM = 2048
EPS = 1e-06
OWN = 56
CHUNKS = 4
LOWEST = -1e30
TP = "tp"
SP = "sp"
BF = jnp.bfloat16
F32 = jnp.float32
INTERPRET = False


V, H, S, A = pltpu.VMEM, pltpu.HBM, pltpu.SMEM, None


def call(kernel, outs, *args, flops=0, scratch=(), places, limit=OWN):
    if not INTERPRET:
        args = [a if p in (S, A) else pltpu.with_memory_space_constraint(a, p) for a, p in zip(args, places)]
    outs = [jax.ShapeDtypeStruct(s, d) if p is A or INTERPRET else p(s, d) for s, d, p in outs]
    return pl.pallas_call(
        kernel,
        out_shape=outs,
        in_specs=[pl.BlockSpec(memory_space=V if p is A else p) for p in places],
        out_specs=[pl.BlockSpec(memory_space=V) for _ in outs],
        scratch_shapes=scratch,
        interpret=INTERPRET,
        compiler_params=pltpu.CompilerParams(vmem_limit_bytes=limit * 2**20),
        cost_estimate=pl.CostEstimate(flops=flops, bytes_accessed=flops // 1000, transcendentals=0) if flops else None,
    )(*args)


def iota(dim):
    return lax.broadcasted_iota(jnp.int32, (N, N), dim)


def to_row(col):
    return jnp.sum(jnp.where(iota(0) == iota(1), col, 0.0), axis=0, keepdims=True)


def to_col(row):
    return jnp.sum(jnp.where(iota(0) == iota(1), row, 0.0), axis=1, keepdims=True)


def pieces(x):
    hi = x.astype(BF)
    rest = x - hi.astype(F32)
    mid = rest.astype(BF)
    low = (rest - mid.astype(F32)).astype(BF)
    return hi, mid, low


def dot(a, b):
    return jnp.dot(a, b, preferred_element_type=F32)


def dot_two(a, b):
    hi = a.astype(BF)
    return dot(hi, b) + dot((a - hi.astype(F32)).astype(BF), b)


def fetched(pairs, sems):
    copies = [pltpu.make_async_copy(src, dst, sems.at[at]) for at, (src, dst) in enumerate(pairs)]
    for c in copies:
        c.start()
    return copies


def prepare(tok_hbm, gain_hbm, out, tok, gain, sems):
    for c in fetched([(tok_hbm, tok), (gain_hbm, gain)], sems):
        c.wait()
    wide = tok[...].astype(F32)
    out[0, :N, :] = (wide * gain[...].astype(F32)).astype(BF)
    squares = to_row(jnp.sum(wide * wide, axis=1, keepdims=True))
    hi, mid, low = pieces(squares)
    zero = jnp.zeros((13, N), F32)
    tail = jnp.concatenate([hi.astype(F32), mid.astype(F32), low.astype(F32), zero], axis=0)
    out[0, N:, :N] = tail.astype(BF)
    out[0, N:, N:] = jnp.zeros((16, N), BF)


def cuts(sources, places):
    step = places[0].shape[0] // CHUNKS
    cut = [pl.ds(c * step, step) for c in range(CHUNKS)]
    return [(s.at[at, :], p.at[at, :]) for at in cut for s, p in zip(sources, places)]


def products(tok, places, copies):
    groups, _, part = tok.shape
    sums = [jnp.zeros((N, p.shape[1]), F32) for p in places]
    for c in range(CHUNKS):
        for each in copies[c * len(places) : (c + 1) * len(places)]:
            each.wait()
        for g in range(c * groups // CHUNKS, (c + 1) * groups // CHUNKS):
            piece = tok[g, :N, :]
            at = pl.ds(g * part, part)
            sums = [s + dot(piece, p[at, :]) for s, p in zip(sums, places)]
    return sums


def log_sigmoid(x):
    e = jnp.exp(-jnp.abs(x))
    series = e * (1.0 - e * (0.5 - e * (1.0 / 3.0 - e * 0.25)))
    return -(jnp.maximum(-x, 0.0) + jnp.where(e < 0.01, series, jnp.log(1.0 + e)))


def states(tok, kw_hbm, vw_hbm, gw_hbm, bias_hbm, message, kv, aux, state, kw, vw, gw, bias, first, sems):
    groups, _, part = tok.shape
    small = fetched([(gw_hbm, gw), (bias_hbm, bias)], first)
    copies = fetched(cuts((kw_hbm, vw_hbm), (kw, vw)), sems)
    for c in small:
        c.wait()
    g_sum = jnp.zeros((N, 2), F32)
    sq = jnp.zeros((1, N), F32)
    for g in range(groups):
        at = pl.ds(g * part, part)
        g_sum += lax.dot_general(tok[g, :N, :], gw[:, at], (((1,), (1,)), ((), ())), preferred_element_type=F32)
        tail = tok[g, N:, :N].astype(F32)
        sq += tail[0:1] + tail[1:2] + tail[2:3]
    inv = lax.rsqrt(to_col(sq) / (groups * part) + EPS)
    gates = inv * g_sum
    i_col = gates[:, 0:1] + bias[0:1, 0:1]
    lf_col = log_sigmoid(gates[:, 1:2] + bias[0:1, 1:2])
    lf_row = to_row(lf_col)
    i_row = to_row(i_col)
    lower = iota(1) <= iota(0)
    b_col = jnp.sum(jnp.where(lower, lf_row, 0.0), axis=1, keepdims=True)
    b_row = jnp.sum(jnp.where(iota(0) <= iota(1), lf_col, 0.0), axis=0, keepdims=True)
    b_all = jnp.sum(lf_col, axis=0, keepdims=True)
    after = jnp.sum(jnp.where(iota(1) > iota(0), lf_row, 0.0), axis=1, keepdims=True)
    weight = after + i_col
    top = jnp.max(weight, axis=0, keepdims=True)
    weight = jnp.exp(weight - top)
    k_sum, v_sum = products(tok, (kw, vw), copies)
    k = (inv * k_sum).astype(BF)
    v = (inv * v_sum).astype(BF)
    kv[:, :HD] = k
    kv[:, HD:] = v
    kf = k.astype(F32) * HD**-0.5
    weighted = weight * kf
    hi = weighted.astype(BF)
    low = (weighted - hi.astype(F32)).astype(BF)
    across = (((0,), (0,)), ((), ()))
    memory = lax.dot_general(hi, v, across, preferred_element_type=F32)
    memory += lax.dot_general(low, v, across, preferred_element_type=F32)
    normer = jnp.sum(weighted, axis=0, keepdims=True)
    lane = lax.broadcasted_iota(jnp.int32, (1, N), 1)
    n_low = normer - normer.astype(BF).astype(F32)
    line = n_low[:, N:]
    for at, p in enumerate(pieces(b_all) + pieces(top)):
        line = jnp.where(lane == at, p.astype(F32), line)
    count, cut = message.shape[0], HD // message.shape[0]
    state[:, 0:cut, :] = memory[:, :N].reshape(count, cut, N)
    state[:, cut : 2 * cut, :] = memory[:, N:].reshape(count, cut, N)
    rest = jnp.concatenate([normer[:, :N], normer[:, N:], line, n_low[:, :N]], axis=0)
    state[:, 2 * cut :, :] = jnp.broadcast_to(rest[None], (count, 4, N))
    message[...] = state[...].astype(BF)
    aux[...] = jnp.concatenate([b_row, i_row, to_row(inv), jnp.zeros((5, N), F32)], axis=0)


def carry(place, arrived, message, own, state, back):
    count, rows, _ = arrived.shape
    slab = rows - 4
    state[...] = arrived[...].astype(F32)
    source = lax.broadcasted_iota(jnp.int32, (count, count), 1)
    target = lax.broadcasted_iota(jnp.int32, (count, count), 0)
    lines = state[:, slab + 2, :]
    tops = lines[:, 3:4] + lines[:, 4:5] + lines[:, 5:6]
    tops = jnp.sum(jnp.where(source == target, tops, 0.0), axis=0, keepdims=True)
    later = jnp.where(source < target, 1.0, 0.0)
    past = later.astype(BF)
    decay = jnp.zeros((count, count), F32)
    for p in range(3):
        decay += dot(past, (later * lines[:, p : p + 1]).astype(BF))
    logs = jnp.where(source < target, tops + decay, LOWEST)
    top = jnp.max(logs, axis=1, keepdims=True)
    weights = jnp.where(source < target, jnp.exp(logs - top), 0.0)
    hi = weights.astype(BF)
    low = (weights - hi.astype(F32)).astype(BF)
    mine = lax.broadcasted_iota(jnp.int32, (count, 1), 0) == place[0]
    pick = lambda a: jnp.sum(jnp.where(mine, a, 0.0), axis=0, keepdims=True)
    lines = []
    lane = lax.broadcasted_iota(jnp.int32, (1, N), 1)
    for r in range(rows):
        part = state[:, r, :]
        part = (jnp.where(lane < 6, 0.0, part) if r == slab + 2 else part).astype(BF)
        whole = dot(hi, part) + dot(low, part)
        if r < slab:
            back[:, r, :] = whole
        else:
            lines.append(pick(whole))
    message[...] = back[...].astype(BF)
    lines = [lines[0] + lines[3], lines[1] + lines[2], jnp.broadcast_to(pick(top), (1, N))]
    own[...] = jnp.concatenate(lines + [jnp.zeros((5, N), F32)], axis=0)


def mixing(tok, aux, bw_hbm, cw_hbm, uw_hbm, gate_b, mixed, edge, bw, cw, uw, sems):
    copies = fetched(cuts((bw_hbm, cw_hbm, uw_hbm), (bw, cw, uw)), sems)
    inv = to_col(aux[2:3, :])
    gb, gc, gu = [(inv * s).astype(BF) for s in products(tok, (bw, cw, uw), copies)]
    gate_b[...] = gb
    mix = (gc.astype(F32) * gu.astype(F32)).astype(BF)
    mixed[...] = mix
    edge[...] = mix[N - 16 :]


def inside(tok, aux, kv, qw_hbm, ow_hbm, gain, pack, qw, ow, sems):
    copies = fetched(cuts((qw_hbm, ow_hbm), (qw, ow)), sems)
    b_row, i_row = aux[0:1, :], aux[1:2, :]
    inv = to_col(aux[2:3, :])
    q, og = [(inv * s).astype(BF) for s in products(tok, (qw, ow), copies)]
    pack[:, :HD] = q.astype(F32)
    pack[:, 2 * HD : 3 * HD] = jax.nn.sigmoid(og.astype(F32)) * gain[...].astype(F32).reshape(1, HD)
    b_col = to_col(b_row)
    causal = iota(1) <= iota(0)
    decays = jnp.where(causal, b_col - b_row + i_row, LOWEST)
    top = jnp.max(decays, axis=1, keepdims=True)
    weights = jnp.where(causal, jnp.exp(decays - top), 0.0)
    scores = lax.dot_general(q, kv[:, :HD], (((1,), (1,)), ((), ())), preferred_element_type=F32)
    scores = scores * HD**-0.5 * weights
    pack[:, HD : 2 * HD] = dot_two(scores, kv[:, HD:])
    denom = jnp.sum(scores, axis=1, keepdims=True)
    lane = iota(1)
    pack[:, 3 * HD :] = jnp.where(lane == 0, b_col, jnp.where(lane == 1, top, jnp.where(lane == 2, denom, 0.0)))


def convolve(place, halo, mixed, gate_b, taps, weight, keep, send):
    now = mixed[...].astype(F32)
    prev = halo[...].astype(F32)[14:]
    row = iota(0)
    one = jnp.where(row == 0, prev[1:2], pltpu.roll(now, 1, 0))
    two = jnp.where(row == 0, prev[0:1], jnp.where(row == 1, prev[1:2], pltpu.roll(now, 2, 0)))
    t = taps[...].astype(F32)
    total = t[0:1] * two + t[1:2] * one + t[2:3] * now
    y = (gate_b[...].astype(F32) * total).astype(BF)
    done = dot(y, weight[...]).astype(BF)
    half = done.shape[1] // 2
    left, right = done[:, :half], done[:, half:]
    first = place[0] % 2 == 0
    keep[...] = jnp.where(first, left, right)
    send[...] = jnp.where(first, right, left)


def finish(arrived, own, pack, keep, other, weight, out, state):
    _, rows, _ = arrived.shape
    half = rows // 2
    q = pack[:, :HD].astype(BF)
    state[...] = arrived[...].astype(F32)
    left = state[:, :half, :].reshape(HD, N).astype(BF)
    right = state[:, half:, :].reshape(HD, N).astype(BF)
    past = jnp.concatenate([dot(q, left), dot(q, right)], axis=1)
    past_den = jnp.sum(pack[:, :N] * own[0:1, :] + pack[:, N:HD] * own[1:2, :], axis=1, keepdims=True)
    cols = pack[:, 3 * HD :]
    b_col, top, denom = cols[:, 0:1], cols[:, 1:2], cols[:, 2:3]
    inter = b_col + own[2:3, 0:1]
    most = jnp.maximum(inter, top)
    old, new = jnp.exp(inter - most), jnp.exp(top - most)
    den = old * past_den + new * denom
    raw = (old * past + new * pack[:, HD : 2 * HD]) / jnp.maximum(jnp.abs(den), jnp.exp(-most))
    squares = jnp.sum(raw * raw, axis=1, keepdims=True)
    y = (pack[:, 2 * HD : 3 * HD] * raw).astype(BF)
    done = dot(y, weight[...]).astype(BF)
    parts = [p.astype(F32) for p in pieces(squares)]
    lane = iota(1)
    tail = jnp.where(lane == 0, parts[0], jnp.where(lane == 1, parts[1], jnp.where(lane == 2, parts[2], 0.0)))
    tail = tail.astype(BF)
    groups, size, _ = out.shape
    width = weight.shape[1]
    conv = (keep[...].astype(F32) + other[...].astype(F32)).astype(BF)
    for g in range(groups):
        at = slice(g * size, (g + 1) * size)
        out[g, :, :width] = done[at]
        out[g, :, width : width + width // 2] = conv[at]
        out[g, :, width + width // 2 :] = tail[at]


def gather_up(arrived, out):
    groups, size, width = arrived.shape
    half = (width - N) // 3
    squares = jnp.zeros((size, 1), F32)
    for g in range(groups):
        tail = arrived[g, :, 3 * half :].astype(F32)
        squares += tail[:, 0:1] + tail[:, 1:2] + tail[:, 2:3]
    scale = lax.rsqrt(squares / MDIM + EPS)
    for side in range(2):
        at = slice(side * half, (side + 1) * half)
        m = jnp.zeros((size, half), F32)
        c = jnp.zeros((size, half), F32)
        for g in range(groups):
            m += arrived[g, :, at].astype(F32)
        for g in range(side, groups, 2):
            c += arrived[g, :, 2 * half : 3 * half].astype(F32)
        out[:, at] = (c + scale * m).astype(BF)


def exchange(value, axis):
    return lax.all_to_all(value, axis, split_axis=0, concat_axis=0, tiled=True)


def body(tokens, norm_gain, conv_b_w, conv_c_w, conv_u_w, conv_taps, query_w, key_w, value_w, outgate_w,
         gate_w, gate_bias, mem_gain, conv_out_w, mem_out_w):
    model = key_w.shape[0]
    count = lax.axis_size(SP)
    groups = lax.axis_size(TP)
    rows = 2 * HD // count
    vmem, hbm = pl.BlockSpec(memory_space=pltpu.VMEM), pl.BlockSpec(memory_space=pltpu.HBM)
    room = lambda *arrays: [pltpu.VMEM(a.shape, a.dtype) for a in arrays]
    sems = lambda n: [pltpu.SemaphoreType.DMA((n,))]
    room = lambda *arrays: [pltpu.VMEM(a.shape, a.dtype) for a in arrays]
    sems = lambda *ns: [pltpu.SemaphoreType.DMA((n,)) for n in ns]
    (local,) = call(
        prepare, [((1, N + 16, tokens.shape[1]), BF, V)], tokens, norm_gain, places=[H, H],
        scratch=room(tokens, norm_gain) + sems(2),
    )
    tok = lax.all_gather(local, TP, axis=0, tiled=True)
    taken = (key_w, value_w, gate_w.reshape(model, 2).T, gate_bias.reshape(1, 2))
    message, kv, aux = call(
        states,
        [((count, rows + 4, N), BF, A), ((N, 2 * HD), BF, A), ((8, N), F32, A)],
        tok, *taken, flops=10**9, places=[V, H, H, H, H],
        scratch=[pltpu.VMEM((count, rows + 4, N), F32)] + room(*taken) + sems(2, 2 * CHUNKS),
    )
    arrived = exchange(message, SP)
    taken = (conv_b_w, conv_c_w, conv_u_w)
    gate_b, mixed, edge = call(
        mixing, [((N, N), BF, V), ((N, N), BF, V), ((16, N), BF, V)], tok, aux, *taken, flops=10**9,
        places=[V, A, H, H, H], scratch=room(*taken) + sems(3 * CHUNKS),
    )
    halo = lax.ppermute(edge, SP, [(i, i + 1) for i in range(count - 1)])
    (pack,) = call(
        inside, [((N, 3 * HD + N), F32, A)], tok, aux, kv, query_w, outgate_w, mem_gain, flops=10**9,
        places=[V, A, A, H, H, A], scratch=room(query_w, outgate_w) + sems(2 * CHUNKS),
    )
    core = lax.axis_index(TP).reshape(1).astype(jnp.int32)
    keep, send = call(
        convolve, [((N, model // 2), BF, V), ((N, model // 2), BF, V)],
        core, halo, mixed, gate_b, conv_taps, conv_out_w,
        flops=10**9, places=[S, V, V, V, A, V], limit=16,
    )
    other = lax.ppermute(send, TP, [(i, i ^ 1) for i in range(groups)])
    place = lax.axis_index(SP).reshape(1).astype(jnp.int32)
    back, own = call(
        carry,
        [((count, rows, N), BF, V), ((8, N), F32, V)],
        place, arrived, flops=10**9, places=[S, V], limit=16,
        scratch=[pltpu.VMEM((count, rows + 4, N), F32), pltpu.VMEM((count, rows, N), F32)],
    )
    state = exchange(back, SP)
    (mem,) = call(
        finish, [((groups, N // groups, 3 * model // 2 + N), BF, V)], state, own, pack, keep, other, mem_out_w,
        flops=10**9, scratch=[pltpu.VMEM((count, rows, N), F32)], places=[V] * 6, limit=16,
    )
    mem = exchange(mem, TP)
    (out,) = call(gather_up, [((N // groups, model), BF, A)], mem, places=[V], limit=16)
    return out


def solution(mesh):
    sp = mesh.shape["sp"]
    finer = Mesh(mesh.devices.reshape(sp, mesh.shape["tp"]), ("sp", "tp"))
    cols = P(None, TP)
    in_specs = (
        P(SP, TP), cols, cols, cols, cols, cols, cols, cols, cols, cols,
        P(None, None, TP), cols, P(TP), P(TP, None), P(TP, None),
    )
    return jax.shard_map(body, mesh=finer, in_specs=in_specs, out_specs=P((SP, TP), None), check_vma=False)
```

```python
import jax
import jax.numpy as jnp
from jax import lax
from jax.experimental import pallas as pl
from jax.experimental.pallas import tpu as pltpu
from jax.sharding import Mesh
from jax.sharding import PartitionSpec as P


N = 128
HD = 256
MDIM = 2048
EPS = 1e-06
OWN = 56
CHUNKS = 4
LOWEST = -1e30
TP = "tp"
SP = "sp"
BF = jnp.bfloat16
F32 = jnp.float32
INTERPRET = False


V, H, S, A = pltpu.VMEM, pltpu.HBM, pltpu.SMEM, None


def call(kernel, outs, *args, flops=0, scratch=(), places, limit=OWN):
    if not INTERPRET:
        args = [a if p in (S, A) else pltpu.with_memory_space_constraint(a, p) for a, p in zip(args, places)]
    outs = [jax.ShapeDtypeStruct(s, d) if p is A or INTERPRET else p(s, d) for s, d, p in outs]
    return pl.pallas_call(
        kernel,
        out_shape=outs,
        in_specs=[pl.BlockSpec(memory_space=V if p is A else p) for p in places],
        out_specs=[pl.BlockSpec(memory_space=V) for _ in outs],
        scratch_shapes=scratch,
        interpret=INTERPRET,
        compiler_params=pltpu.CompilerParams(vmem_limit_bytes=limit * 2**20),
        cost_estimate=pl.CostEstimate(flops=flops, bytes_accessed=flops // 1000, transcendentals=0) if flops else None,
    )(*args)


def iota(dim):
    return lax.broadcasted_iota(jnp.int32, (N, N), dim)


def to_row(col):
    return jnp.sum(jnp.where(iota(0) == iota(1), col, 0.0), axis=0, keepdims=True)


def to_col(row):
    return jnp.sum(jnp.where(iota(0) == iota(1), row, 0.0), axis=1, keepdims=True)


def pieces(x):
    hi = x.astype(BF)
    rest = x - hi.astype(F32)
    mid = rest.astype(BF)
    low = (rest - mid.astype(F32)).astype(BF)
    return hi, mid, low


def dot(a, b):
    return jnp.dot(a, b, preferred_element_type=F32)


def dot_two(a, b):
    hi = a.astype(BF)
    return dot(hi, b) + dot((a - hi.astype(F32)).astype(BF), b)


def fetched(pairs, sems):
    copies = [pltpu.make_async_copy(src, dst, sems.at[at]) for at, (src, dst) in enumerate(pairs)]
    for c in copies:
        c.start()
    return copies


def prepare(tok_hbm, gain_hbm, gw_hbm, bias_hbm, taps_hbm, out, gw, bias, taps, tok, gain, sems):
    for c in fetched([(tok_hbm, tok), (gain_hbm, gain), (gw_hbm, gw), (bias_hbm, bias), (taps_hbm, taps)], sems):
        c.wait()
    wide = tok[...].astype(F32)
    out[0, :N, :] = (wide * gain[...].astype(F32)).astype(BF)
    squares = to_row(jnp.sum(wide * wide, axis=1, keepdims=True))
    hi, mid, low = pieces(squares)
    zero = jnp.zeros((13, N), F32)
    tail = jnp.concatenate([hi.astype(F32), mid.astype(F32), low.astype(F32), zero], axis=0)
    out[0, N:, :N] = tail.astype(BF)
    out[0, N:, N:] = jnp.zeros((16, N), BF)


def cuts(sources, places):
    step = places[0].shape[0] // CHUNKS
    cut = [pl.ds(c * step, step) for c in range(CHUNKS)]
    return [(s.at[at, :], p.at[at, :]) for at in cut for s, p in zip(sources, places)]


def products(tok, places, copies=()):
    groups, _, part = tok.shape
    sums = [jnp.zeros((N, p.shape[1]), F32) for p in places]
    for c in range(CHUNKS):
        for each in copies[c * len(places) : (c + 1) * len(places)]:
            each.wait()
        for g in range(c * groups // CHUNKS, (c + 1) * groups // CHUNKS):
            piece = tok[g, :N, :]
            at = pl.ds(g * part, part)
            sums = [s + dot(piece, p[at, :]) for s, p in zip(sums, places)]
    return sums


def log_sigmoid(x):
    e = jnp.exp(-jnp.abs(x))
    series = e * (1.0 - e * (0.5 - e * (1.0 / 3.0 - e * 0.25)))
    return -(jnp.maximum(-x, 0.0) + jnp.where(e < 0.01, series, jnp.log(1.0 + e)))


def states(tok, gw, bias, kw_hbm, vw_hbm, message, kv, aux, state, kw, vw, sems):
    groups, _, part = tok.shape
    copies = fetched(cuts((kw_hbm, vw_hbm), (kw, vw)), sems)
    g_sum = jnp.zeros((N, 2), F32)
    sq = jnp.zeros((1, N), F32)
    for g in range(groups):
        at = pl.ds(g * part, part)
        g_sum += lax.dot_general(tok[g, :N, :], gw[:, at], (((1,), (1,)), ((), ())), preferred_element_type=F32)
        tail = tok[g, N:, :N].astype(F32)
        sq += tail[0:1] + tail[1:2] + tail[2:3]
    inv = lax.rsqrt(to_col(sq) / (groups * part) + EPS)
    gates = inv * g_sum
    i_col = gates[:, 0:1] + bias[0:1, 0:1]
    lf_col = log_sigmoid(gates[:, 1:2] + bias[0:1, 1:2])
    lf_row = to_row(lf_col)
    i_row = to_row(i_col)
    lower = iota(1) <= iota(0)
    b_col = jnp.sum(jnp.where(lower, lf_row, 0.0), axis=1, keepdims=True)
    b_row = jnp.sum(jnp.where(iota(0) <= iota(1), lf_col, 0.0), axis=0, keepdims=True)
    b_all = jnp.sum(lf_col, axis=0, keepdims=True)
    after = jnp.sum(jnp.where(iota(1) > iota(0), lf_row, 0.0), axis=1, keepdims=True)
    weight = after + i_col
    top = jnp.max(weight, axis=0, keepdims=True)
    weight = jnp.exp(weight - top)
    k_sum, v_sum = products(tok, (kw, vw), copies)
    k = (inv * k_sum).astype(BF)
    v = (inv * v_sum).astype(BF)
    kv[:, :HD] = k
    kv[:, HD:] = v
    kf = k.astype(F32) * HD**-0.5
    weighted = weight * kf
    hi = weighted.astype(BF)
    low = (weighted - hi.astype(F32)).astype(BF)
    across = (((0,), (0,)), ((), ()))
    memory = lax.dot_general(hi, v, across, preferred_element_type=F32)
    memory += lax.dot_general(low, v, across, preferred_element_type=F32)
    normer = jnp.sum(weighted, axis=0, keepdims=True)
    lane = lax.broadcasted_iota(jnp.int32, (1, N), 1)
    n_low = normer - normer.astype(BF).astype(F32)
    line = n_low[:, N:]
    for at, p in enumerate(pieces(b_all) + pieces(top)):
        line = jnp.where(lane == at, p.astype(F32), line)
    count, cut = message.shape[0], HD // message.shape[0]
    state[:, 0:cut, :] = memory[:, :N].reshape(count, cut, N)
    state[:, cut : 2 * cut, :] = memory[:, N:].reshape(count, cut, N)
    rest = jnp.concatenate([normer[:, :N], normer[:, N:], line, n_low[:, :N]], axis=0)
    state[:, 2 * cut :, :] = jnp.broadcast_to(rest[None], (count, 4, N))
    message[...] = state[...].astype(BF)
    aux[...] = jnp.concatenate([b_row, i_row, to_row(inv), jnp.zeros((5, N), F32)], axis=0)


def carry(place, arrived, _, message, own, state, back):
    count, rows, _ = arrived.shape
    slab = rows - 4
    state[...] = arrived[...].astype(F32)
    source = lax.broadcasted_iota(jnp.int32, (count, count), 1)
    target = lax.broadcasted_iota(jnp.int32, (count, count), 0)
    lines = state[:, slab + 2, :]
    tops = lines[:, 3:4] + lines[:, 4:5] + lines[:, 5:6]
    tops = jnp.sum(jnp.where(source == target, tops, 0.0), axis=0, keepdims=True)
    later = jnp.where(source < target, 1.0, 0.0)
    past = later.astype(BF)
    decay = jnp.zeros((count, count), F32)
    for p in range(3):
        decay += dot(past, (later * lines[:, p : p + 1]).astype(BF))
    logs = jnp.where(source < target, tops + decay, LOWEST)
    top = jnp.max(logs, axis=1, keepdims=True)
    weights = jnp.where(source < target, jnp.exp(logs - top), 0.0)
    hi = weights.astype(BF)
    low = (weights - hi.astype(F32)).astype(BF)
    mine = lax.broadcasted_iota(jnp.int32, (count, 1), 0) == place[0]
    pick = lambda a: jnp.sum(jnp.where(mine, a, 0.0), axis=0, keepdims=True)
    lane = lax.broadcasted_iota(jnp.int32, (1, N), 1)
    parts = [state[:, r, :] for r in range(rows)]
    parts[slab + 2] = jnp.where(lane < 6, 0.0, parts[slab + 2])
    wide = jnp.concatenate([p.astype(BF) for p in parts], axis=1)
    whole = dot(jnp.concatenate([hi, low], axis=1), jnp.concatenate([wide, wide], axis=0))
    whole = [whole[:, r * N : (r + 1) * N] for r in range(rows)]
    for r in range(slab):
        back[:, r, :] = whole[r]
    message[...] = back[...].astype(BF)
    lines = [pick(w) for w in whole[slab:]]
    lines = [lines[0] + lines[3], lines[1] + lines[2], jnp.broadcast_to(pick(top), (1, N))]
    own[...] = jnp.concatenate(lines + [jnp.zeros((5, N), F32)], axis=0)


def mixing(tok, aux, bw, cw, uw, gate_b, mixed, edge):
    inv = to_col(aux[2:3, :])
    gb, gc, gu = [(inv * s).astype(BF) for s in products(tok, (bw, cw, uw))]
    gate_b[...] = gb
    mix = (gc.astype(F32) * gu.astype(F32)).astype(BF)
    mixed[...] = mix
    edge[...] = mix[N - 16 :]


def inside(tok, aux, kv, qw_hbm, ow_hbm, gain, pack, qw, ow, sems):
    copies = fetched(cuts((qw_hbm, ow_hbm), (qw, ow)), sems)
    b_row, i_row = aux[0:1, :], aux[1:2, :]
    inv = to_col(aux[2:3, :])
    q, og = [(inv * s).astype(BF) for s in products(tok, (qw, ow), copies)]
    pack[:, :HD] = q.astype(F32)
    pack[:, 2 * HD : 3 * HD] = jax.nn.sigmoid(og.astype(F32)) * gain[...].astype(F32).reshape(1, HD)
    b_col = to_col(b_row)
    causal = iota(1) <= iota(0)
    decays = jnp.where(causal, b_col - b_row + i_row, LOWEST)
    top = jnp.max(decays, axis=1, keepdims=True)
    weights = jnp.where(causal, jnp.exp(decays - top), 0.0)
    scores = lax.dot_general(q, kv[:, :HD], (((1,), (1,)), ((), ())), preferred_element_type=F32)
    scores = scores * HD**-0.5 * weights
    pack[:, HD : 2 * HD] = dot_two(scores, kv[:, HD:])
    denom = jnp.sum(scores, axis=1, keepdims=True)
    lane = iota(1)
    pack[:, 3 * HD :] = jnp.where(lane == 0, b_col, jnp.where(lane == 1, top, jnp.where(lane == 2, denom, 0.0)))


def convolve(place, halo, mixed, gate_b, taps, weight, keep, send):
    now = mixed[...].astype(F32)
    prev = halo[...].astype(F32)[14:]
    row = iota(0)
    one = jnp.where(row == 0, prev[1:2], pltpu.roll(now, 1, 0))
    two = jnp.where(row == 0, prev[0:1], jnp.where(row == 1, prev[1:2], pltpu.roll(now, 2, 0)))
    t = taps[...].astype(F32)
    total = t[0:1] * two + t[1:2] * one + t[2:3] * now
    y = (gate_b[...].astype(F32) * total).astype(BF)
    done = dot(y, weight[...]).astype(BF)
    half = done.shape[1] // 2
    left, right = done[:, :half], done[:, half:]
    first = place[0] % 2 == 0
    keep[...] = jnp.where(first, left, right)
    send[...] = jnp.where(first, right, left)


def finish(arrived, own, pack, keep, other, weight, out, state):
    _, rows, _ = arrived.shape
    half = rows // 2
    q = pack[:, :HD].astype(BF)
    state[...] = arrived[...].astype(F32)
    left = state[:, :half, :].reshape(HD, N).astype(BF)
    right = state[:, half:, :].reshape(HD, N).astype(BF)
    past = jnp.concatenate([dot(q, left), dot(q, right)], axis=1)
    past_den = jnp.sum(pack[:, :N] * own[0:1, :] + pack[:, N:HD] * own[1:2, :], axis=1, keepdims=True)
    cols = pack[:, 3 * HD :]
    b_col, top, denom = cols[:, 0:1], cols[:, 1:2], cols[:, 2:3]
    inter = b_col + own[2:3, 0:1]
    most = jnp.maximum(inter, top)
    old, new = jnp.exp(inter - most), jnp.exp(top - most)
    den = old * past_den + new * denom
    raw = (old * past + new * pack[:, HD : 2 * HD]) / jnp.maximum(jnp.abs(den), jnp.exp(-most))
    squares = jnp.sum(raw * raw, axis=1, keepdims=True)
    y = (pack[:, 2 * HD : 3 * HD] * raw).astype(BF)
    done = dot(y, weight[...]).astype(BF)
    parts = [p.astype(F32) for p in pieces(squares)]
    lane = iota(1)
    tail = jnp.where(lane == 0, parts[0], jnp.where(lane == 1, parts[1], jnp.where(lane == 2, parts[2], 0.0)))
    tail = tail.astype(BF)
    groups, size, _ = out.shape
    width = weight.shape[1]
    conv = (keep[...].astype(F32) + other[...].astype(F32)).astype(BF)
    for g in range(groups):
        at = slice(g * size, (g + 1) * size)
        out[g, :, :width] = done[at]
        out[g, :, width : width + width // 2] = conv[at]
        out[g, :, width + width // 2 :] = tail[at]


def gather_up(arrived, out):
    groups, size, width = arrived.shape
    half = (width - N) // 3
    squares = jnp.zeros((size, 1), F32)
    for g in range(groups):
        tail = arrived[g, :, 3 * half :].astype(F32)
        squares += tail[:, 0:1] + tail[:, 1:2] + tail[:, 2:3]
    scale = lax.rsqrt(squares / MDIM + EPS)
    for side in range(2):
        at = slice(side * half, (side + 1) * half)
        m = jnp.zeros((size, half), F32)
        c = jnp.zeros((size, half), F32)
        for g in range(groups):
            m += arrived[g, :, at].astype(F32)
        for g in range(side, groups, 2):
            c += arrived[g, :, 2 * half : 3 * half].astype(F32)
        out[:, at] = (c + scale * m).astype(BF)


def exchange(value, axis):
    return lax.all_to_all(value, axis, split_axis=0, concat_axis=0, tiled=True)


def body(tokens, norm_gain, conv_b_w, conv_c_w, conv_u_w, conv_taps, query_w, key_w, value_w, outgate_w,
         gate_w, gate_bias, mem_gain, conv_out_w, mem_out_w):
    model = key_w.shape[0]
    count = lax.axis_size(SP)
    groups = lax.axis_size(TP)
    rows = 2 * HD // count
    vmem, hbm = pl.BlockSpec(memory_space=pltpu.VMEM), pl.BlockSpec(memory_space=pltpu.HBM)
    room = lambda *arrays: [pltpu.VMEM(a.shape, a.dtype) for a in arrays]
    sems = lambda n: [pltpu.SemaphoreType.DMA((n,))]
    room = lambda *arrays: [pltpu.VMEM(a.shape, a.dtype) for a in arrays]
    sems = lambda *ns: [pltpu.SemaphoreType.DMA((n,)) for n in ns]
    small = (gate_w.reshape(model, 2).T, gate_bias.reshape(1, 2), conv_taps)
    local, gate_wt, biases, taps = call(
        prepare,
        [((1, N + 16, tokens.shape[1]), BF, V)] + [(a.shape, a.dtype, V) for a in small],
        tokens, norm_gain, *small, places=[H] * 5, scratch=room(tokens, norm_gain) + sems(5),
    )
    tok = lax.all_gather(local, TP, axis=0, tiled=True)
    message, kv, aux = call(
        states,
        [((count, rows + 4, N), BF, A), ((N, 2 * HD), BF, A), ((8, N), F32, V)],
        tok, gate_wt, biases, key_w, value_w, flops=10**9, places=[V, V, V, H, H],
        scratch=[pltpu.VMEM((count, rows + 4, N), F32)] + room(key_w, value_w) + sems(2 * CHUNKS),
    )
    arrived = exchange(message, SP)
    gate_b, mixed, edge = call(
        mixing, [((N, N), BF, V), ((N, N), BF, V), ((16, N), BF, V)], tok, aux, conv_b_w, conv_c_w,
        conv_u_w, flops=10**9, places=[V] * 5, limit=16,
    )
    halo = lax.ppermute(edge, SP, [(i, i + 1) for i in range(count - 1)])
    (pack,) = call(
        inside, [((N, 3 * HD + N), F32, A)], tok, aux, kv, query_w, outgate_w, mem_gain, flops=10**9,
        places=[V, V, A, H, H, A], scratch=room(query_w, outgate_w) + sems(2 * CHUNKS),
    )
    core = lax.axis_index(TP).reshape(1).astype(jnp.int32)
    keep, send = call(
        convolve, [((N, model // 2), BF, V), ((N, model // 2), BF, V)],
        core, halo, mixed, gate_b, taps, conv_out_w,
        flops=10**9, places=[S] + [V] * 5, limit=16,
    )
    other = lax.ppermute(send, TP, [(i, i ^ 1) for i in range(groups)])
    place = lax.axis_index(SP).reshape(1).astype(jnp.int32)
    back, own = call(
        carry,
        [((count, rows, N), BF, V), ((8, N), F32, V)],
        place, arrived, other, flops=10**9, places=[S, V, V], limit=16,
        scratch=[pltpu.VMEM((count, rows + 4, N), F32), pltpu.VMEM((count, rows, N), F32)],
    )
    state = exchange(back, SP)
    (mem,) = call(
        finish, [((groups, N // groups, 3 * model // 2 + N), BF, V)], state, own, pack, keep, other, mem_out_w,
        flops=10**9, scratch=[pltpu.VMEM((count, rows, N), F32)], places=[V] * 6, limit=16,
    )
    mem = exchange(mem, TP)
    (out,) = call(gather_up, [((N // groups, model), BF, A)], mem, places=[V], limit=16)
    return out


def solution(mesh):
    sp = mesh.shape["sp"]
    finer = Mesh(mesh.devices.reshape(sp, mesh.shape["tp"]), ("sp", "tp"))
    cols = P(None, TP)
    in_specs = (
        P(SP, TP), cols, cols, cols, cols, cols, cols, cols, cols, cols,
        P(None, None, TP), cols, P(TP), P(TP, None), P(TP, None),
    )
    return jax.shard_map(body, mesh=finer, in_specs=in_specs, out_specs=P((SP, TP), None), check_vma=False)
```

```python
import jax
import jax.numpy as jnp
from jax import lax
from jax.experimental import pallas as pl
from jax.experimental.pallas import tpu as pltpu
from jax.sharding import Mesh
from jax.sharding import PartitionSpec as P


N = 128
HD = 256
MDIM = 2048
EPS = 1e-06
OWN = 56
CHUNKS = 4
LOWEST = -1e30
TP = "tp"
SP = "sp"
BF = jnp.bfloat16
F32 = jnp.float32
INTERPRET = False


V, H, S, A = pltpu.VMEM, pltpu.HBM, pltpu.SMEM, None


def call(kernel, outs, *args, flops=0, scratch=(), places, limit=OWN):
    if not INTERPRET:
        args = [a if p in (S, A) else pltpu.with_memory_space_constraint(a, p) for a, p in zip(args, places)]
    outs = [jax.ShapeDtypeStruct(s, d) if p is A or INTERPRET else p(s, d) for s, d, p in outs]
    return pl.pallas_call(
        kernel,
        out_shape=outs,
        in_specs=[pl.BlockSpec(memory_space=V if p is A else p) for p in places],
        out_specs=[pl.BlockSpec(memory_space=V) for _ in outs],
        scratch_shapes=scratch,
        interpret=INTERPRET,
        compiler_params=pltpu.CompilerParams(vmem_limit_bytes=limit * 2**20),
        cost_estimate=pl.CostEstimate(flops=flops, bytes_accessed=flops // 1000, transcendentals=0) if flops else None,
    )(*args)


def iota(dim):
    return lax.broadcasted_iota(jnp.int32, (N, N), dim)


def to_row(col):
    return jnp.sum(jnp.where(iota(0) == iota(1), col, 0.0), axis=0, keepdims=True)


def to_col(row):
    return jnp.sum(jnp.where(iota(0) == iota(1), row, 0.0), axis=1, keepdims=True)


def pieces(x):
    hi = x.astype(BF)
    rest = x - hi.astype(F32)
    mid = rest.astype(BF)
    low = (rest - mid.astype(F32)).astype(BF)
    return hi, mid, low


def dot(a, b):
    return jnp.dot(a, b, preferred_element_type=F32)


def dot_two(a, b):
    hi = a.astype(BF)
    return dot(hi, b) + dot((a - hi.astype(F32)).astype(BF), b)


def fetched(pairs, sems):
    copies = [pltpu.make_async_copy(src, dst, sems.at[at]) for at, (src, dst) in enumerate(pairs)]
    for c in copies:
        c.start()
    return copies


def prepare(tok_hbm, gain_hbm, *rest):
    count = (len(rest) - 4) // 2
    sources, out, places, (tok, gain, sems) = rest[:count], rest[count], rest[count + 1 : -3], rest[-3:]
    copies = fetched([(tok_hbm, tok), (gain_hbm, gain), *zip(sources, places)], sems)
    copies[0].wait()
    copies[1].wait()
    wide = tok[...].astype(F32)
    out[0, :N, :] = (wide * gain[...].astype(F32)).astype(BF)
    squares = to_row(jnp.sum(wide * wide, axis=1, keepdims=True))
    hi, mid, low = pieces(squares)
    zero = jnp.zeros((13, N), F32)
    tail = jnp.concatenate([hi.astype(F32), mid.astype(F32), low.astype(F32), zero], axis=0)
    out[0, N:, :N] = tail.astype(BF)
    out[0, N:, N:] = jnp.zeros((16, N), BF)
    for c in copies[2:]:
        c.wait()


def cuts(sources, places):
    step = places[0].shape[0] // CHUNKS
    cut = [pl.ds(c * step, step) for c in range(CHUNKS)]
    return [(s.at[at, :], p.at[at, :]) for at in cut for s, p in zip(sources, places)]


def products(tok, places, copies=()):
    groups, _, part = tok.shape
    sums = [jnp.zeros((N, p.shape[1]), F32) for p in places]
    for c in range(CHUNKS):
        for each in copies[c * len(places) : (c + 1) * len(places)]:
            each.wait()
        for g in range(c * groups // CHUNKS, (c + 1) * groups // CHUNKS):
            piece = tok[g, :N, :]
            at = pl.ds(g * part, part)
            sums = [s + dot(piece, p[at, :]) for s, p in zip(sums, places)]
    return sums


def log_sigmoid(x):
    e = jnp.exp(-jnp.abs(x))
    series = e * (1.0 - e * (0.5 - e * (1.0 / 3.0 - e * 0.25)))
    return -(jnp.maximum(-x, 0.0) + jnp.where(e < 0.01, series, jnp.log(1.0 + e)))


def states(tok, gw, bias, kw, vw, message, kv, aux, state):
    groups, _, part = tok.shape
    g_sum = jnp.zeros((N, 2), F32)
    sq = jnp.zeros((1, N), F32)
    for g in range(groups):
        at = pl.ds(g * part, part)
        g_sum += lax.dot_general(tok[g, :N, :], gw[:, at], (((1,), (1,)), ((), ())), preferred_element_type=F32)
        tail = tok[g, N:, :N].astype(F32)
        sq += tail[0:1] + tail[1:2] + tail[2:3]
    inv = lax.rsqrt(to_col(sq) / (groups * part) + EPS)
    gates = inv * g_sum
    i_col = gates[:, 0:1] + bias[0:1, 0:1]
    lf_col = log_sigmoid(gates[:, 1:2] + bias[0:1, 1:2])
    lf_row = to_row(lf_col)
    i_row = to_row(i_col)
    lower = iota(1) <= iota(0)
    b_col = jnp.sum(jnp.where(lower, lf_row, 0.0), axis=1, keepdims=True)
    b_row = jnp.sum(jnp.where(iota(0) <= iota(1), lf_col, 0.0), axis=0, keepdims=True)
    b_all = jnp.sum(lf_col, axis=0, keepdims=True)
    after = jnp.sum(jnp.where(iota(1) > iota(0), lf_row, 0.0), axis=1, keepdims=True)
    weight = after + i_col
    top = jnp.max(weight, axis=0, keepdims=True)
    weight = jnp.exp(weight - top)
    k_sum, v_sum = products(tok, (kw, vw))
    k = (inv * k_sum).astype(BF)
    v = (inv * v_sum).astype(BF)
    kv[:, :HD] = k
    kv[:, HD:] = v
    kf = k.astype(F32) * HD**-0.5
    weighted = weight * kf
    hi = weighted.astype(BF)
    low = (weighted - hi.astype(F32)).astype(BF)
    across = (((0,), (0,)), ((), ()))
    memory = lax.dot_general(hi, v, across, preferred_element_type=F32)
    memory += lax.dot_general(low, v, across, preferred_element_type=F32)
    normer = jnp.sum(weighted, axis=0, keepdims=True)
    lane = lax.broadcasted_iota(jnp.int32, (1, N), 1)
    n_low = normer - normer.astype(BF).astype(F32)
    line = n_low[:, N:]
    for at, p in enumerate(pieces(b_all) + pieces(top)):
        line = jnp.where(lane == at, p.astype(F32), line)
    count, cut = message.shape[0], HD // message.shape[0]
    state[:, 0:cut, :] = memory[:, :N].reshape(count, cut, N)
    state[:, cut : 2 * cut, :] = memory[:, N:].reshape(count, cut, N)
    rest = jnp.concatenate([normer[:, :N], normer[:, N:], line, n_low[:, :N]], axis=0)
    state[:, 2 * cut :, :] = jnp.broadcast_to(rest[None], (count, 4, N))
    message[...] = state[...].astype(BF)
    aux[...] = jnp.concatenate([b_row, i_row, to_row(inv), jnp.zeros((5, N), F32)], axis=0)


def carry(place, arrived, message, own, state, back):
    count, rows, _ = arrived.shape
    slab = rows - 4
    state[...] = arrived[...].astype(F32)
    source = lax.broadcasted_iota(jnp.int32, (count, count), 1)
    target = lax.broadcasted_iota(jnp.int32, (count, count), 0)
    lines = state[:, slab + 2, :]
    tops = lines[:, 3:4] + lines[:, 4:5] + lines[:, 5:6]
    tops = jnp.sum(jnp.where(source == target, tops, 0.0), axis=0, keepdims=True)
    later = jnp.where(source < target, 1.0, 0.0)
    past = later.astype(BF)
    decay = jnp.zeros((count, count), F32)
    for p in range(3):
        decay += dot(past, (later * lines[:, p : p + 1]).astype(BF))
    logs = jnp.where(source < target, tops + decay, LOWEST)
    top = jnp.max(logs, axis=1, keepdims=True)
    weights = jnp.where(source < target, jnp.exp(logs - top), 0.0)
    hi = weights.astype(BF)
    low = (weights - hi.astype(F32)).astype(BF)
    mine = lax.broadcasted_iota(jnp.int32, (count, 1), 0) == place[0]
    pick = lambda a: jnp.sum(jnp.where(mine, a, 0.0), axis=0, keepdims=True)
    lane = lax.broadcasted_iota(jnp.int32, (1, N), 1)
    parts = [state[:, r, :] for r in range(rows)]
    parts[slab + 2] = jnp.where(lane < 6, 0.0, parts[slab + 2])
    wide = jnp.concatenate([p.astype(BF) for p in parts], axis=1)
    whole = dot(jnp.concatenate([hi, low], axis=1), jnp.concatenate([wide, wide], axis=0))
    whole = [whole[:, r * N : (r + 1) * N] for r in range(rows)]
    for r in range(slab):
        back[:, r, :] = whole[r]
    message[...] = back[...].astype(BF)
    lines = [pick(w) for w in whole[slab:]]
    lines = [lines[0] + lines[3], lines[1] + lines[2], jnp.broadcast_to(pick(top), (1, N))]
    own[...] = jnp.concatenate(lines + [jnp.zeros((5, N), F32)], axis=0)


def mixing(tok, aux, bw, cw, uw, gate_b, mixed, edge):
    inv = to_col(aux[2:3, :])
    gb, gc, gu = [(inv * s).astype(BF) for s in products(tok, (bw, cw, uw))]
    gate_b[...] = gb
    mix = (gc.astype(F32) * gu.astype(F32)).astype(BF)
    mixed[...] = mix
    edge[...] = mix[N - 16 :]


def inside(tok, aux, kv, qw_hbm, ow_hbm, gain, pack, qw, ow, sems):
    copies = fetched(cuts((qw_hbm, ow_hbm), (qw, ow)), sems)
    b_row, i_row = aux[0:1, :], aux[1:2, :]
    inv = to_col(aux[2:3, :])
    q, og = [(inv * s).astype(BF) for s in products(tok, (qw, ow), copies)]
    pack[:, :HD] = q.astype(F32)
    pack[:, 2 * HD : 3 * HD] = jax.nn.sigmoid(og.astype(F32)) * gain[...].astype(F32).reshape(1, HD)
    b_col = to_col(b_row)
    causal = iota(1) <= iota(0)
    decays = jnp.where(causal, b_col - b_row + i_row, LOWEST)
    top = jnp.max(decays, axis=1, keepdims=True)
    weights = jnp.where(causal, jnp.exp(decays - top), 0.0)
    scores = lax.dot_general(q, kv[:, :HD], (((1,), (1,)), ((), ())), preferred_element_type=F32)
    scores = scores * HD**-0.5 * weights
    pack[:, HD : 2 * HD] = dot_two(scores, kv[:, HD:])
    denom = jnp.sum(scores, axis=1, keepdims=True)
    lane = iota(1)
    pack[:, 3 * HD :] = jnp.where(lane == 0, b_col, jnp.where(lane == 1, top, jnp.where(lane == 2, denom, 0.0)))


def convolve(place, halo, mixed, gate_b, taps, weight, keep, send):
    now = mixed[...].astype(F32)
    prev = halo[...].astype(F32)[14:]
    row = iota(0)
    one = jnp.where(row == 0, prev[1:2], pltpu.roll(now, 1, 0))
    two = jnp.where(row == 0, prev[0:1], jnp.where(row == 1, prev[1:2], pltpu.roll(now, 2, 0)))
    t = taps[...].astype(F32)
    total = t[0:1] * two + t[1:2] * one + t[2:3] * now
    y = (gate_b[...].astype(F32) * total).astype(BF)
    done = dot(y, weight[...]).astype(BF)
    half = done.shape[1] // 2
    left, right = done[:, :half], done[:, half:]
    first = place[0] % 2 == 0
    keep[...] = jnp.where(first, left, right)
    send[...] = jnp.where(first, right, left)


def finish(arrived, own, pack, keep, other, weight, out, state):
    _, rows, _ = arrived.shape
    half = rows // 2
    q = pack[:, :HD].astype(BF)
    state[...] = arrived[...].astype(F32)
    left = state[:, :half, :].reshape(HD, N).astype(BF)
    right = state[:, half:, :].reshape(HD, N).astype(BF)
    past = jnp.concatenate([dot(q, left), dot(q, right)], axis=1)
    past_den = jnp.sum(pack[:, :N] * own[0:1, :] + pack[:, N:HD] * own[1:2, :], axis=1, keepdims=True)
    cols = pack[:, 3 * HD :]
    b_col, top, denom = cols[:, 0:1], cols[:, 1:2], cols[:, 2:3]
    inter = b_col + own[2:3, 0:1]
    most = jnp.maximum(inter, top)
    old, new = jnp.exp(inter - most), jnp.exp(top - most)
    den = old * past_den + new * denom
    raw = (old * past + new * pack[:, HD : 2 * HD]) / jnp.maximum(jnp.abs(den), jnp.exp(-most))
    squares = jnp.sum(raw * raw, axis=1, keepdims=True)
    y = (pack[:, 2 * HD : 3 * HD] * raw).astype(BF)
    done = dot(y, weight[...]).astype(BF)
    parts = [p.astype(F32) for p in pieces(squares)]
    lane = iota(1)
    tail = jnp.where(lane == 0, parts[0], jnp.where(lane == 1, parts[1], jnp.where(lane == 2, parts[2], 0.0)))
    tail = tail.astype(BF)
    groups, size, _ = out.shape
    width = weight.shape[1]
    conv = (keep[...].astype(F32) + other[...].astype(F32)).astype(BF)
    for g in range(groups):
        at = slice(g * size, (g + 1) * size)
        out[g, :, :width] = done[at]
        out[g, :, width : width + width // 2] = conv[at]
        out[g, :, width + width // 2 :] = tail[at]


def gather_up(arrived, out):
    groups, size, width = arrived.shape
    half = (width - N) // 3
    squares = jnp.zeros((size, 1), F32)
    for g in range(groups):
        tail = arrived[g, :, 3 * half :].astype(F32)
        squares += tail[:, 0:1] + tail[:, 1:2] + tail[:, 2:3]
    scale = lax.rsqrt(squares / MDIM + EPS)
    for side in range(2):
        at = slice(side * half, (side + 1) * half)
        m = jnp.zeros((size, half), F32)
        c = jnp.zeros((size, half), F32)
        for g in range(groups):
            m += arrived[g, :, at].astype(F32)
        for g in range(side, groups, 2):
            c += arrived[g, :, 2 * half : 3 * half].astype(F32)
        out[:, at] = (c + scale * m).astype(BF)


def exchange(value, axis):
    return lax.all_to_all(value, axis, split_axis=0, concat_axis=0, tiled=True)


def body(tokens, norm_gain, conv_b_w, conv_c_w, conv_u_w, conv_taps, query_w, key_w, value_w, outgate_w,
         gate_w, gate_bias, mem_gain, conv_out_w, mem_out_w):
    model = key_w.shape[0]
    count = lax.axis_size(SP)
    groups = lax.axis_size(TP)
    rows = 2 * HD // count
    vmem, hbm = pl.BlockSpec(memory_space=pltpu.VMEM), pl.BlockSpec(memory_space=pltpu.HBM)
    room = lambda *arrays: [pltpu.VMEM(a.shape, a.dtype) for a in arrays]
    sems = lambda n: [pltpu.SemaphoreType.DMA((n,))]
    room = lambda *arrays: [pltpu.VMEM(a.shape, a.dtype) for a in arrays]
    sems = lambda *ns: [pltpu.SemaphoreType.DMA((n,)) for n in ns]
    small = (gate_w.reshape(model, 2).T, gate_bias.reshape(1, 2), conv_taps, key_w, value_w)
    local, gate_wt, biases, taps, key_v, value_v = call(
        prepare,
        [((1, N + 16, tokens.shape[1]), BF, V)] + [(a.shape, a.dtype, V) for a in small],
        tokens, norm_gain, *small, places=[H] * 7, scratch=room(tokens, norm_gain) + sems(7),
    )
    tok = lax.all_gather(local, TP, axis=0, tiled=True)
    message, kv, aux = call(
        states,
        [((count, rows + 4, N), BF, A), ((N, 2 * HD), BF, A), ((8, N), F32, V)],
        tok, gate_wt, biases, key_v, value_v, flops=10**9, places=[V] * 5,
        scratch=[pltpu.VMEM((count, rows + 4, N), F32)],
    )
    arrived = exchange(message, SP)
    gate_b, mixed, edge = call(
        mixing, [((N, N), BF, V), ((N, N), BF, V), ((16, N), BF, V)], tok, aux, conv_b_w, conv_c_w,
        conv_u_w, flops=10**9, places=[V] * 5, limit=16,
    )
    halo = lax.ppermute(edge, SP, [(i, i + 1) for i in range(count - 1)])
    (pack,) = call(
        inside, [((N, 3 * HD + N), F32, A)], tok, aux, kv, query_w, outgate_w, mem_gain, flops=10**9,
        places=[V, V, A, H, H, A], scratch=room(query_w, outgate_w) + sems(2 * CHUNKS),
    )
    core = lax.axis_index(TP).reshape(1).astype(jnp.int32)
    keep, send = call(
        convolve, [((N, model // 2), BF, V), ((N, model // 2), BF, V)],
        core, halo, mixed, gate_b, taps, conv_out_w,
        flops=10**9, places=[S] + [V] * 5, limit=16,
    )
    other = lax.ppermute(send, TP, [(i, i ^ 1) for i in range(groups)])
    place = lax.axis_index(SP).reshape(1).astype(jnp.int32)
    back, own = call(
        carry,
        [((count, rows, N), BF, V), ((8, N), F32, V)],
        place, arrived, flops=10**9, places=[S, V], limit=16,
        scratch=[pltpu.VMEM((count, rows + 4, N), F32), pltpu.VMEM((count, rows, N), F32)],
    )
    state = exchange(back, SP)
    (mem,) = call(
        finish, [((groups, N // groups, 3 * model // 2 + N), BF, V)], state, own, pack, keep, other, mem_out_w,
        flops=10**9, scratch=[pltpu.VMEM((count, rows, N), F32)], places=[V] * 6, limit=16,
    )
    mem = exchange(mem, TP)
    (out,) = call(gather_up, [((N // groups, model), BF, A)], mem, places=[V], limit=16)
    return out


def solution(mesh):
    sp = mesh.shape["sp"]
    finer = Mesh(mesh.devices.reshape(sp, mesh.shape["tp"]), ("sp", "tp"))
    cols = P(None, TP)
    in_specs = (
        P(SP, TP), cols, cols, cols, cols, cols, cols, cols, cols, cols,
        P(None, None, TP), cols, P(TP), P(TP, None), P(TP, None),
    )
    return jax.shard_map(body, mesh=finer, in_specs=in_specs, out_specs=P((SP, TP), None), check_vma=False)
```

```python
import jax
import jax.numpy as jnp
from jax import lax
from jax.experimental import pallas as pl
from jax.experimental.pallas import tpu as pltpu
from jax.sharding import Mesh
from jax.sharding import PartitionSpec as P


N = 128
HD = 256
MDIM = 2048
EPS = 1e-06
OWN = 56
FIRST = 84
CHUNKS = 4
LOWEST = -1e30
TP = "tp"
SP = "sp"
BF = jnp.bfloat16
F32 = jnp.float32
INTERPRET = False


V, H, S, A = pltpu.VMEM, pltpu.HBM, pltpu.SMEM, None


def call(kernel, outs, *args, flops=0, scratch=(), places, limit=OWN):
    if not INTERPRET:
        args = [a if p in (S, A) else pltpu.with_memory_space_constraint(a, p) for a, p in zip(args, places)]
    outs = [jax.ShapeDtypeStruct(s, d) if p is A or INTERPRET else p(s, d) for s, d, p in outs]
    return pl.pallas_call(
        kernel,
        out_shape=outs,
        in_specs=[pl.BlockSpec(memory_space=V if p is A else p) for p in places],
        out_specs=[pl.BlockSpec(memory_space=V) for _ in outs],
        scratch_shapes=scratch,
        interpret=INTERPRET,
        compiler_params=pltpu.CompilerParams(vmem_limit_bytes=limit * 2**20),
        cost_estimate=pl.CostEstimate(flops=flops, bytes_accessed=flops // 1000, transcendentals=0) if flops else None,
    )(*args)


def iota(dim):
    return lax.broadcasted_iota(jnp.int32, (N, N), dim)


def to_row(col):
    return jnp.sum(jnp.where(iota(0) == iota(1), col, 0.0), axis=0, keepdims=True)


def to_col(row):
    return jnp.sum(jnp.where(iota(0) == iota(1), row, 0.0), axis=1, keepdims=True)


def pieces(x):
    hi = x.astype(BF)
    rest = x - hi.astype(F32)
    mid = rest.astype(BF)
    low = (rest - mid.astype(F32)).astype(BF)
    return hi, mid, low


def dot(a, b):
    return jnp.dot(a, b, preferred_element_type=F32)


def dot_two(a, b):
    hi = a.astype(BF)
    return dot(hi, b) + dot((a - hi.astype(F32)).astype(BF), b)


def fetched(pairs, sems):
    copies = [pltpu.make_async_copy(src, dst, sems.at[at]) for at, (src, dst) in enumerate(pairs)]
    for c in copies:
        c.start()
    return copies


def prepare(tok_hbm, gain_hbm, *rest):
    count = (len(rest) - 4) // 2
    sources, out, places, (tok, gain, sems) = rest[:count], rest[count], rest[count + 1 : -3], rest[-3:]
    copies = fetched([(tok_hbm, tok), (gain_hbm, gain), *zip(sources, places)], sems)
    copies[0].wait()
    copies[1].wait()
    wide = tok[...].astype(F32)
    out[0, :N, :] = (wide * gain[...].astype(F32)).astype(BF)
    squares = to_row(jnp.sum(wide * wide, axis=1, keepdims=True))
    hi, mid, low = pieces(squares)
    zero = jnp.zeros((13, N), F32)
    tail = jnp.concatenate([hi.astype(F32), mid.astype(F32), low.astype(F32), zero], axis=0)
    out[0, N:, :N] = tail.astype(BF)
    out[0, N:, N:] = jnp.zeros((16, N), BF)
    for c in copies[2:]:
        c.wait()


def cuts(sources, places):
    step = places[0].shape[0] // CHUNKS
    cut = [pl.ds(c * step, step) for c in range(CHUNKS)]
    return [(s.at[at, :], p.at[at, :]) for at in cut for s, p in zip(sources, places)]


def products(tok, places, copies=()):
    groups, _, part = tok.shape
    sums = [jnp.zeros((N, p.shape[1]), F32) for p in places]
    for c in range(CHUNKS):
        for each in copies[c * len(places) : (c + 1) * len(places)]:
            each.wait()
        for g in range(c * groups // CHUNKS, (c + 1) * groups // CHUNKS):
            piece = tok[g, :N, :]
            at = pl.ds(g * part, part)
            sums = [s + dot(piece, p[at, :]) for s, p in zip(sums, places)]
    return sums


def log_sigmoid(x):
    e = jnp.exp(-jnp.abs(x))
    series = e * (1.0 - e * (0.5 - e * (1.0 / 3.0 - e * 0.25)))
    return -(jnp.maximum(-x, 0.0) + jnp.where(e < 0.01, series, jnp.log(1.0 + e)))


def states(tok, gw, bias, kw, vw, message, kv, aux, state):
    groups, _, part = tok.shape
    g_sum = jnp.zeros((N, 2), F32)
    sq = jnp.zeros((1, N), F32)
    for g in range(groups):
        at = pl.ds(g * part, part)
        g_sum += lax.dot_general(tok[g, :N, :], gw[:, at], (((1,), (1,)), ((), ())), preferred_element_type=F32)
        tail = tok[g, N:, :N].astype(F32)
        sq += tail[0:1] + tail[1:2] + tail[2:3]
    inv = lax.rsqrt(to_col(sq) / (groups * part) + EPS)
    gates = inv * g_sum
    i_col = gates[:, 0:1] + bias[0:1, 0:1]
    lf_col = log_sigmoid(gates[:, 1:2] + bias[0:1, 1:2])
    lf_row = to_row(lf_col)
    i_row = to_row(i_col)
    lower = iota(1) <= iota(0)
    b_col = jnp.sum(jnp.where(lower, lf_row, 0.0), axis=1, keepdims=True)
    b_row = jnp.sum(jnp.where(iota(0) <= iota(1), lf_col, 0.0), axis=0, keepdims=True)
    b_all = jnp.sum(lf_col, axis=0, keepdims=True)
    after = jnp.sum(jnp.where(iota(1) > iota(0), lf_row, 0.0), axis=1, keepdims=True)
    weight = after + i_col
    top = jnp.max(weight, axis=0, keepdims=True)
    weight = jnp.exp(weight - top)
    k_sum, v_sum = products(tok, (kw, vw))
    k = (inv * k_sum).astype(BF)
    v = (inv * v_sum).astype(BF)
    kv[:, :HD] = k
    kv[:, HD:] = v
    kf = k.astype(F32) * HD**-0.5
    weighted = weight * kf
    hi = weighted.astype(BF)
    low = (weighted - hi.astype(F32)).astype(BF)
    across = (((0,), (0,)), ((), ()))
    memory = lax.dot_general(hi, v, across, preferred_element_type=F32)
    memory += lax.dot_general(low, v, across, preferred_element_type=F32)
    normer = jnp.sum(weighted, axis=0, keepdims=True)
    lane = lax.broadcasted_iota(jnp.int32, (1, N), 1)
    n_low = normer - normer.astype(BF).astype(F32)
    line = n_low[:, N:]
    for at, p in enumerate(pieces(b_all) + pieces(top)):
        line = jnp.where(lane == at, p.astype(F32), line)
    count, cut = message.shape[0], HD // message.shape[0]
    state[:, 0:cut, :] = memory[:, :N].reshape(count, cut, N)
    state[:, cut : 2 * cut, :] = memory[:, N:].reshape(count, cut, N)
    rest = jnp.concatenate([normer[:, :N], normer[:, N:], line, n_low[:, :N]], axis=0)
    state[:, 2 * cut :, :] = jnp.broadcast_to(rest[None], (count, 4, N))
    message[...] = state[...].astype(BF)
    aux[...] = jnp.concatenate([b_row, i_row, to_row(inv), jnp.zeros((5, N), F32)], axis=0)


def carry(place, arrived, message, own, state, back):
    count, rows, _ = arrived.shape
    slab = rows - 4
    state[...] = arrived[...].astype(F32)
    column = lax.broadcasted_iota(jnp.int32, (count, count), 1)
    line = lax.broadcasted_iota(jnp.int32, (count, count), 0)
    source, target = (column + FIRST) % count, (line + FIRST) % count
    lines = state[:, slab + 2, :]
    tops = lines[:, 3:4] + lines[:, 4:5] + lines[:, 5:6]
    tops = jnp.sum(jnp.where(column == line, tops, 0.0), axis=0, keepdims=True)
    later = jnp.where(source < target, 1.0, 0.0)
    past = later.astype(BF)
    decay = jnp.zeros((count, count), F32)
    for p in range(3):
        decay += dot(past, (later * lines[:, p : p + 1]).astype(BF))
    logs = jnp.where(source < target, tops + decay, LOWEST)
    top = jnp.max(logs, axis=1, keepdims=True)
    weights = jnp.where(source < target, jnp.exp(logs - top), 0.0)
    hi = weights.astype(BF)
    low = (weights - hi.astype(F32)).astype(BF)
    mine = (lax.broadcasted_iota(jnp.int32, (count, 1), 0) + FIRST) % count == place[0]
    pick = lambda a: jnp.sum(jnp.where(mine, a, 0.0), axis=0, keepdims=True)
    lane = lax.broadcasted_iota(jnp.int32, (1, N), 1)
    parts = [state[:, r, :] for r in range(rows)]
    parts[slab + 2] = jnp.where(lane < 6, 0.0, parts[slab + 2])
    wide = jnp.concatenate([p.astype(BF) for p in parts], axis=1)
    whole = dot(jnp.concatenate([hi, low], axis=1), jnp.concatenate([wide, wide], axis=0))
    whole = [whole[:, r * N : (r + 1) * N] for r in range(rows)]
    for r in range(slab):
        back[:, r, :] = whole[r]
    message[...] = back[...].astype(BF)
    lines = [pick(w) for w in whole[slab:]]
    lines = [lines[0] + lines[3], lines[1] + lines[2], jnp.broadcast_to(pick(top), (1, N))]
    own[...] = jnp.concatenate(lines + [jnp.zeros((5, N), F32)], axis=0)


def mixing(tok, aux, bw, cw, uw, gate_b, mixed, edge):
    inv = to_col(aux[2:3, :])
    gb, gc, gu = [(inv * s).astype(BF) for s in products(tok, (bw, cw, uw))]
    gate_b[...] = gb
    mix = (gc.astype(F32) * gu.astype(F32)).astype(BF)
    mixed[...] = mix
    edge[...] = mix[N - 16 :]


def inside(tok, aux, kv, qw_hbm, ow_hbm, gain, pack, qw, ow, sems):
    copies = fetched(cuts((qw_hbm, ow_hbm), (qw, ow)), sems)
    b_row, i_row = aux[0:1, :], aux[1:2, :]
    inv = to_col(aux[2:3, :])
    q, og = [(inv * s).astype(BF) for s in products(tok, (qw, ow), copies)]
    pack[:, :HD] = q.astype(F32)
    pack[:, 2 * HD : 3 * HD] = jax.nn.sigmoid(og.astype(F32)) * gain[...].astype(F32).reshape(1, HD)
    b_col = to_col(b_row)
    causal = iota(1) <= iota(0)
    decays = jnp.where(causal, b_col - b_row + i_row, LOWEST)
    top = jnp.max(decays, axis=1, keepdims=True)
    weights = jnp.where(causal, jnp.exp(decays - top), 0.0)
    scores = lax.dot_general(q, kv[:, :HD], (((1,), (1,)), ((), ())), preferred_element_type=F32)
    scores = scores * HD**-0.5 * weights
    pack[:, HD : 2 * HD] = dot_two(scores, kv[:, HD:])
    denom = jnp.sum(scores, axis=1, keepdims=True)
    lane = iota(1)
    pack[:, 3 * HD :] = jnp.where(lane == 0, b_col, jnp.where(lane == 1, top, jnp.where(lane == 2, denom, 0.0)))


def convolve(place, halo, mixed, gate_b, taps, weight, keep, send):
    now = mixed[...].astype(F32)
    prev = halo[...].astype(F32)[14:]
    row = iota(0)
    one = jnp.where(row == 0, prev[1:2], pltpu.roll(now, 1, 0))
    two = jnp.where(row == 0, prev[0:1], jnp.where(row == 1, prev[1:2], pltpu.roll(now, 2, 0)))
    t = taps[...].astype(F32)
    total = t[0:1] * two + t[1:2] * one + t[2:3] * now
    y = (gate_b[...].astype(F32) * total).astype(BF)
    done = dot(y, weight[...]).astype(BF)
    half = done.shape[1] // 2
    left, right = done[:, :half], done[:, half:]
    first = place[0] % 2 == 0
    keep[...] = jnp.where(first, left, right)
    send[...] = jnp.where(first, right, left)


def finish(arrived, own, pack, keep, other, weight, out, state):
    _, rows, _ = arrived.shape
    half = rows // 2
    q = pack[:, :HD].astype(BF)
    state[...] = arrived[...].astype(F32)
    left = state[:, :half, :].reshape(HD, N).astype(BF)
    right = state[:, half:, :].reshape(HD, N).astype(BF)
    past = jnp.concatenate([dot(q, left), dot(q, right)], axis=1)
    past_den = jnp.sum(pack[:, :N] * own[0:1, :] + pack[:, N:HD] * own[1:2, :], axis=1, keepdims=True)
    cols = pack[:, 3 * HD :]
    b_col, top, denom = cols[:, 0:1], cols[:, 1:2], cols[:, 2:3]
    inter = b_col + own[2:3, 0:1]
    most = jnp.maximum(inter, top)
    old, new = jnp.exp(inter - most), jnp.exp(top - most)
    den = old * past_den + new * denom
    raw = (old * past + new * pack[:, HD : 2 * HD]) / jnp.maximum(jnp.abs(den), jnp.exp(-most))
    squares = jnp.sum(raw * raw, axis=1, keepdims=True)
    y = (pack[:, 2 * HD : 3 * HD] * raw).astype(BF)
    done = dot(y, weight[...]).astype(BF)
    parts = [p.astype(F32) for p in pieces(squares)]
    lane = iota(1)
    tail = jnp.where(lane == 0, parts[0], jnp.where(lane == 1, parts[1], jnp.where(lane == 2, parts[2], 0.0)))
    tail = tail.astype(BF)
    groups, size, _ = out.shape
    width = weight.shape[1]
    conv = (keep[...].astype(F32) + other[...].astype(F32)).astype(BF)
    for g in range(groups):
        at = slice(g * size, (g + 1) * size)
        out[g, :, :width] = done[at]
        out[g, :, width : width + width // 2] = conv[at]
        out[g, :, width + width // 2 :] = tail[at]


def gather_up(arrived, out):
    groups, size, width = arrived.shape
    half = (width - N) // 3
    squares = jnp.zeros((size, 1), F32)
    for g in range(groups):
        tail = arrived[g, :, 3 * half :].astype(F32)
        squares += tail[:, 0:1] + tail[:, 1:2] + tail[:, 2:3]
    scale = lax.rsqrt(squares / MDIM + EPS)
    for side in range(2):
        at = slice(side * half, (side + 1) * half)
        m = jnp.zeros((size, half), F32)
        c = jnp.zeros((size, half), F32)
        for g in range(groups):
            m += arrived[g, :, at].astype(F32)
        for g in range(side, groups, 2):
            c += arrived[g, :, 2 * half : 3 * half].astype(F32)
        out[:, at] = (c + scale * m).astype(BF)


def exchange(value, axis, first=0):
    count = lax.axis_size(axis)
    order = [[(i + first) % count for i in range(count)]] if first else None
    return lax.all_to_all(value, axis, split_axis=0, concat_axis=0, tiled=True, axis_index_groups=order)


def body(tokens, norm_gain, conv_b_w, conv_c_w, conv_u_w, conv_taps, query_w, key_w, value_w, outgate_w,
         gate_w, gate_bias, mem_gain, conv_out_w, mem_out_w):
    model = key_w.shape[0]
    count = lax.axis_size(SP)
    groups = lax.axis_size(TP)
    rows = 2 * HD // count
    vmem, hbm = pl.BlockSpec(memory_space=pltpu.VMEM), pl.BlockSpec(memory_space=pltpu.HBM)
    room = lambda *arrays: [pltpu.VMEM(a.shape, a.dtype) for a in arrays]
    sems = lambda n: [pltpu.SemaphoreType.DMA((n,))]
    room = lambda *arrays: [pltpu.VMEM(a.shape, a.dtype) for a in arrays]
    sems = lambda *ns: [pltpu.SemaphoreType.DMA((n,)) for n in ns]
    small = (gate_w.reshape(model, 2).T, gate_bias.reshape(1, 2), conv_taps, key_w, value_w)
    local, gate_wt, biases, taps, key_v, value_v = call(
        prepare,
        [((1, N + 16, tokens.shape[1]), BF, V)] + [(a.shape, a.dtype, V) for a in small],
        tokens, norm_gain, *small, places=[H] * 7, scratch=room(tokens, norm_gain) + sems(7),
    )
    tok = lax.all_gather(local, TP, axis=0, tiled=True)
    message, kv, aux = call(
        states,
        [((count, rows + 4, N), BF, A), ((N, 2 * HD), BF, A), ((8, N), F32, V)],
        tok, gate_wt, biases, key_v, value_v, flops=10**9, places=[V] * 5,
        scratch=[pltpu.VMEM((count, rows + 4, N), F32)],
    )
    arrived = exchange(message, SP, FIRST % count)
    gate_b, mixed, edge = call(
        mixing, [((N, N), BF, V), ((N, N), BF, V), ((16, N), BF, V)], tok, aux, conv_b_w, conv_c_w,
        conv_u_w, flops=10**9, places=[V] * 5, limit=16,
    )
    halo = lax.ppermute(edge, SP, [(i, i + 1) for i in range(count - 1)])
    (pack,) = call(
        inside, [((N, 3 * HD + N), F32, A)], tok, aux, kv, query_w, outgate_w, mem_gain, flops=10**9,
        places=[V, V, A, H, H, A], scratch=room(query_w, outgate_w) + sems(2 * CHUNKS),
    )
    core = lax.axis_index(TP).reshape(1).astype(jnp.int32)
    keep, send = call(
        convolve, [((N, model // 2), BF, V), ((N, model // 2), BF, V)],
        core, halo, mixed, gate_b, taps, conv_out_w,
        flops=10**9, places=[S] + [V] * 5, limit=16,
    )
    other = lax.ppermute(send, TP, [(i, i ^ 1) for i in range(groups)])
    place = lax.axis_index(SP).reshape(1).astype(jnp.int32)
    back, own = call(
        carry,
        [((count, rows, N), BF, V), ((8, N), F32, V)],
        place, arrived, flops=10**9, places=[S, V], limit=16,
        scratch=[pltpu.VMEM((count, rows + 4, N), F32), pltpu.VMEM((count, rows, N), F32)],
    )
    state = exchange(back, SP, FIRST % count)
    (mem,) = call(
        finish, [((groups, N // groups, 3 * model // 2 + N), BF, V)], state, own, pack, keep, other, mem_out_w,
        flops=10**9, scratch=[pltpu.VMEM((count, rows, N), F32)], places=[V] * 6, limit=16,
    )
    mem = exchange(mem, TP)
    (out,) = call(gather_up, [((N // groups, model), BF, A)], mem, places=[V], limit=16)
    return out


def solution(mesh):
    sp = mesh.shape["sp"]
    finer = Mesh(mesh.devices.reshape(sp, mesh.shape["tp"]), ("sp", "tp"))
    cols = P(None, TP)
    in_specs = (
        P(SP, TP), cols, cols, cols, cols, cols, cols, cols, cols, cols,
        P(None, None, TP), cols, P(TP), P(TP, None), P(TP, None),
    )
    return jax.shard_map(body, mesh=finer, in_specs=in_specs, out_specs=P((SP, TP), None), check_vma=False)
```

```python
import jax
import jax.numpy as jnp
from jax import lax
from jax.experimental import pallas as pl
from jax.experimental.pallas import tpu as pltpu
from jax.sharding import Mesh
from jax.sharding import PartitionSpec as P


N = 128
HD = 256
MDIM = 2048
EPS = 1e-06
OWN = 56
FIRST = 76
TP_FIRST = 6
CHUNKS = 4
LOWEST = -1e30
TP = "tp"
SP = "sp"
BF = jnp.bfloat16
F32 = jnp.float32
INTERPRET = False


V, H, S, A = pltpu.VMEM, pltpu.HBM, pltpu.SMEM, None


def call(kernel, outs, *args, flops=0, scratch=(), places, limit=OWN):
    if not INTERPRET:
        args = [a if p in (S, A) else pltpu.with_memory_space_constraint(a, p) for a, p in zip(args, places)]
    outs = [jax.ShapeDtypeStruct(s, d) if p is A or INTERPRET else p(s, d) for s, d, p in outs]
    return pl.pallas_call(
        kernel,
        out_shape=outs,
        in_specs=[pl.BlockSpec(memory_space=V if p is A else p) for p in places],
        out_specs=[pl.BlockSpec(memory_space=V) for _ in outs],
        scratch_shapes=scratch,
        interpret=INTERPRET,
        compiler_params=pltpu.CompilerParams(vmem_limit_bytes=limit * 2**20),
        cost_estimate=pl.CostEstimate(flops=flops, bytes_accessed=flops // 1000, transcendentals=0) if flops else None,
    )(*args)


def iota(dim):
    return lax.broadcasted_iota(jnp.int32, (N, N), dim)


def to_row(col):
    return jnp.sum(jnp.where(iota(0) == iota(1), col, 0.0), axis=0, keepdims=True)


def to_col(row):
    return jnp.sum(jnp.where(iota(0) == iota(1), row, 0.0), axis=1, keepdims=True)


def pieces(x):
    hi = x.astype(BF)
    rest = x - hi.astype(F32)
    mid = rest.astype(BF)
    low = (rest - mid.astype(F32)).astype(BF)
    return hi, mid, low


def dot(a, b):
    return jnp.dot(a, b, preferred_element_type=F32)


def dot_two(a, b):
    hi = a.astype(BF)
    return dot(hi, b) + dot((a - hi.astype(F32)).astype(BF), b)


def fetched(pairs, sems):
    copies = [pltpu.make_async_copy(src, dst, sems.at[at]) for at, (src, dst) in enumerate(pairs)]
    for c in copies:
        c.start()
    return copies


def prepare(tok_hbm, gain_hbm, gw_hbm, bias_hbm, taps_hbm, kw_hbm, vw_hbm,
            out, gw, bias, taps, kw, vw, tok, gain, first, sems):
    mine = fetched([(tok_hbm, tok), (gain_hbm, gain)], first)
    small = [(gw_hbm, gw), (bias_hbm, bias), (taps_hbm, taps)]
    others = fetched(small + cuts((kw_hbm, vw_hbm), (kw, vw)), sems)
    for c in mine:
        c.wait()
    wide = tok[...].astype(F32)
    out[0, :N, :] = (wide * gain[...].astype(F32)).astype(BF)
    squares = to_row(jnp.sum(wide * wide, axis=1, keepdims=True))
    hi, mid, low = pieces(squares)
    zero = jnp.zeros((13, N), F32)
    tail = jnp.concatenate([hi.astype(F32), mid.astype(F32), low.astype(F32), zero], axis=0)
    out[0, N:, :N] = tail.astype(BF)
    out[0, N:, N:] = jnp.zeros((16, N), BF)
    for c in others:
        c.wait()


def cuts(sources, places):
    step = places[0].shape[0] // CHUNKS
    cut = [pl.ds(c * step, step) for c in range(CHUNKS)]
    return [(s.at[at, :], p.at[at, :]) for at in cut for s, p in zip(sources, places)]


def products(tok, places, copies=()):
    groups, _, part = tok.shape
    sums = [jnp.zeros((N, p.shape[1]), F32) for p in places]
    for c in range(CHUNKS):
        for each in copies[c * len(places) : (c + 1) * len(places)]:
            each.wait()
        for g in range(c * groups // CHUNKS, (c + 1) * groups // CHUNKS):
            piece = tok[g, :N, :]
            at = pl.ds(g * part, part)
            sums = [s + dot(piece, p[at, :]) for s, p in zip(sums, places)]
    return sums


def log_sigmoid(x):
    e = jnp.exp(-jnp.abs(x))
    series = e * (1.0 - e * (0.5 - e * (1.0 / 3.0 - e * 0.25)))
    return -(jnp.maximum(-x, 0.0) + jnp.where(e < 0.01, series, jnp.log(1.0 + e)))


def states(tok, gw, bias, kw, vw, message, kv, aux, state):
    groups, _, part = tok.shape
    g_sum = jnp.zeros((N, 2), F32)
    sq = jnp.zeros((1, N), F32)
    for g in range(groups):
        at = pl.ds(g * part, part)
        g_sum += lax.dot_general(tok[g, :N, :], gw[:, at], (((1,), (1,)), ((), ())), preferred_element_type=F32)
        tail = tok[g, N:, :N].astype(F32)
        sq += tail[0:1] + tail[1:2] + tail[2:3]
    inv = lax.rsqrt(to_col(sq) / (groups * part) + EPS)
    gates = inv * g_sum
    i_col = gates[:, 0:1] + bias[0:1, 0:1]
    lf_col = log_sigmoid(gates[:, 1:2] + bias[0:1, 1:2])
    lf_row = to_row(lf_col)
    i_row = to_row(i_col)
    lower = iota(1) <= iota(0)
    b_col = jnp.sum(jnp.where(lower, lf_row, 0.0), axis=1, keepdims=True)
    b_row = jnp.sum(jnp.where(iota(0) <= iota(1), lf_col, 0.0), axis=0, keepdims=True)
    b_all = jnp.sum(lf_col, axis=0, keepdims=True)
    after = jnp.sum(jnp.where(iota(1) > iota(0), lf_row, 0.0), axis=1, keepdims=True)
    weight = after + i_col
    top = jnp.max(weight, axis=0, keepdims=True)
    weight = jnp.exp(weight - top)
    k_sum, v_sum = products(tok, (kw, vw))
    k = (inv * k_sum).astype(BF)
    v = (inv * v_sum).astype(BF)
    kv[:, :HD] = k
    kv[:, HD:] = v
    kf = k.astype(F32) * HD**-0.5
    weighted = weight * kf
    hi = weighted.astype(BF)
    low = (weighted - hi.astype(F32)).astype(BF)
    across = (((0,), (0,)), ((), ()))
    memory = lax.dot_general(hi, v, across, preferred_element_type=F32)
    memory += lax.dot_general(low, v, across, preferred_element_type=F32)
    normer = jnp.sum(weighted, axis=0, keepdims=True)
    lane = lax.broadcasted_iota(jnp.int32, (1, N), 1)
    n_low = normer - normer.astype(BF).astype(F32)
    line = n_low[:, N:]
    for at, p in enumerate(pieces(b_all) + pieces(top)):
        line = jnp.where(lane == at, p.astype(F32), line)
    count, cut = message.shape[0], HD // message.shape[0]
    state[:, 0:cut, :] = memory[:, :N].reshape(count, cut, N)
    state[:, cut : 2 * cut, :] = memory[:, N:].reshape(count, cut, N)
    rest = jnp.concatenate([normer[:, :N], normer[:, N:], line, n_low[:, :N]], axis=0)
    state[:, 2 * cut :, :] = jnp.broadcast_to(rest[None], (count, 4, N))
    message[...] = state[...].astype(BF)
    aux[...] = jnp.concatenate([b_row, i_row, to_row(inv), jnp.zeros((5, N), F32)], axis=0)


def carry(place, arrived, message, own, state, back):
    count, rows, _ = arrived.shape
    slab = rows - 4
    state[...] = arrived[...].astype(F32)
    column = lax.broadcasted_iota(jnp.int32, (count, count), 1)
    line = lax.broadcasted_iota(jnp.int32, (count, count), 0)
    source, target = (column + FIRST) % count, (line + FIRST) % count
    lines = state[:, slab + 2, :]
    tops = lines[:, 3:4] + lines[:, 4:5] + lines[:, 5:6]
    tops = jnp.sum(jnp.where(column == line, tops, 0.0), axis=0, keepdims=True)
    later = jnp.where(source < target, 1.0, 0.0)
    past = later.astype(BF)
    decay = jnp.zeros((count, count), F32)
    for p in range(3):
        decay += dot(past, (later * lines[:, p : p + 1]).astype(BF))
    logs = jnp.where(source < target, tops + decay, LOWEST)
    top = jnp.max(logs, axis=1, keepdims=True)
    weights = jnp.where(source < target, jnp.exp(logs - top), 0.0)
    hi = weights.astype(BF)
    low = (weights - hi.astype(F32)).astype(BF)
    mine = (lax.broadcasted_iota(jnp.int32, (count, 1), 0) + FIRST) % count == place[0]
    pick = lambda a: jnp.sum(jnp.where(mine, a, 0.0), axis=0, keepdims=True)
    lane = lax.broadcasted_iota(jnp.int32, (1, N), 1)
    parts = [state[:, r, :] for r in range(rows)]
    parts[slab + 2] = jnp.where(lane < 6, 0.0, parts[slab + 2])
    wide = jnp.concatenate([p.astype(BF) for p in parts], axis=1)
    whole = dot(jnp.concatenate([hi, low], axis=1), jnp.concatenate([wide, wide], axis=0))
    whole = [whole[:, r * N : (r + 1) * N] for r in range(rows)]
    for r in range(slab):
        back[:, r, :] = whole[r]
    message[...] = back[...].astype(BF)
    lines = [pick(w) for w in whole[slab:]]
    lines = [lines[0] + lines[3], lines[1] + lines[2], jnp.broadcast_to(pick(top), (1, N))]
    own[...] = jnp.concatenate(lines + [jnp.zeros((5, N), F32)], axis=0)


def mixing(tok, aux, bw, cw, uw, gate_b, mixed, edge):
    inv = to_col(aux[2:3, :])
    gb, gc, gu = [(inv * s).astype(BF) for s in products(tok, (bw, cw, uw))]
    gate_b[...] = gb
    mix = (gc.astype(F32) * gu.astype(F32)).astype(BF)
    mixed[...] = mix
    edge[...] = mix[N - 16 :]


def inside(tok, aux, kv, qw_hbm, ow_hbm, gain, pack, qw, ow, sems):
    copies = fetched(cuts((qw_hbm, ow_hbm), (qw, ow)), sems)
    b_row, i_row = aux[0:1, :], aux[1:2, :]
    inv = to_col(aux[2:3, :])
    q, og = [(inv * s).astype(BF) for s in products(tok, (qw, ow), copies)]
    pack[:, :HD] = q.astype(F32)
    pack[:, 2 * HD : 3 * HD] = jax.nn.sigmoid(og.astype(F32)) * gain[...].astype(F32).reshape(1, HD)
    b_col = to_col(b_row)
    causal = iota(1) <= iota(0)
    decays = jnp.where(causal, b_col - b_row + i_row, LOWEST)
    top = jnp.max(decays, axis=1, keepdims=True)
    weights = jnp.where(causal, jnp.exp(decays - top), 0.0)
    scores = lax.dot_general(q, kv[:, :HD], (((1,), (1,)), ((), ())), preferred_element_type=F32)
    scores = scores * HD**-0.5 * weights
    pack[:, HD : 2 * HD] = dot_two(scores, kv[:, HD:])
    denom = jnp.sum(scores, axis=1, keepdims=True)
    lane = iota(1)
    pack[:, 3 * HD :] = jnp.where(lane == 0, b_col, jnp.where(lane == 1, top, jnp.where(lane == 2, denom, 0.0)))


def convolve(place, halo, mixed, gate_b, taps, weight, keep, send):
    now = mixed[...].astype(F32)
    prev = halo[...].astype(F32)[14:]
    row = iota(0)
    one = jnp.where(row == 0, prev[1:2], pltpu.roll(now, 1, 0))
    two = jnp.where(row == 0, prev[0:1], jnp.where(row == 1, prev[1:2], pltpu.roll(now, 2, 0)))
    t = taps[...].astype(F32)
    total = t[0:1] * two + t[1:2] * one + t[2:3] * now
    y = (gate_b[...].astype(F32) * total).astype(BF)
    done = dot(y, weight[...]).astype(BF)
    half = done.shape[1] // 2
    left, right = done[:, :half], done[:, half:]
    first = place[0] % 2 == 0
    keep[...] = jnp.where(first, left, right)
    send[...] = jnp.where(first, right, left)


def finish(arrived, own, pack, keep, other, weight, out, state):
    _, rows, _ = arrived.shape
    half = rows // 2
    q = pack[:, :HD].astype(BF)
    state[...] = arrived[...].astype(F32)
    left = state[:, :half, :].reshape(HD, N).astype(BF)
    right = state[:, half:, :].reshape(HD, N).astype(BF)
    past = jnp.concatenate([dot(q, left), dot(q, right)], axis=1)
    past_den = jnp.sum(pack[:, :N] * own[0:1, :] + pack[:, N:HD] * own[1:2, :], axis=1, keepdims=True)
    cols = pack[:, 3 * HD :]
    b_col, top, denom = cols[:, 0:1], cols[:, 1:2], cols[:, 2:3]
    inter = b_col + own[2:3, 0:1]
    most = jnp.maximum(inter, top)
    old, new = jnp.exp(inter - most), jnp.exp(top - most)
    den = old * past_den + new * denom
    raw = (old * past + new * pack[:, HD : 2 * HD]) / jnp.maximum(jnp.abs(den), jnp.exp(-most))
    squares = jnp.sum(raw * raw, axis=1, keepdims=True)
    y = (pack[:, 2 * HD : 3 * HD] * raw).astype(BF)
    done = dot(y, weight[...]).astype(BF)
    parts = [p.astype(F32) for p in pieces(squares)]
    lane = iota(1)
    tail = jnp.where(lane == 0, parts[0], jnp.where(lane == 1, parts[1], jnp.where(lane == 2, parts[2], 0.0)))
    tail = tail.astype(BF)
    groups, size, _ = out.shape
    width = weight.shape[1]
    conv = (keep[...].astype(F32) + other[...].astype(F32)).astype(BF)
    for g in range(groups):
        at = slice(g * size, (g + 1) * size)
        to = (g - TP_FIRST) % groups
        out[to, :, :width] = done[at]
        out[to, :, width : width + width // 2] = conv[at]
        out[to, :, width + width // 2 :] = tail[at]


def gather_up(arrived, out):
    groups, size, width = arrived.shape
    half = (width - N) // 3
    squares = jnp.zeros((size, 1), F32)
    for g in range(groups):
        tail = arrived[g, :, 3 * half :].astype(F32)
        squares += tail[:, 0:1] + tail[:, 1:2] + tail[:, 2:3]
    scale = lax.rsqrt(squares / MDIM + EPS)
    for side in range(2):
        at = slice(side * half, (side + 1) * half)
        m = jnp.zeros((size, half), F32)
        c = jnp.zeros((size, half), F32)
        for g in range(groups):
            m += arrived[g, :, at].astype(F32)
        for g in range((side - TP_FIRST) % 2, groups, 2):
            c += arrived[g, :, 2 * half : 3 * half].astype(F32)
        out[:, at] = (c + scale * m).astype(BF)


def exchange(value, axis, first=0):
    count = lax.axis_size(axis)
    order = [[(i + first) % count for i in range(count)]] if first else None
    return lax.all_to_all(value, axis, split_axis=0, concat_axis=0, tiled=True, axis_index_groups=order)


def body(tokens, norm_gain, conv_b_w, conv_c_w, conv_u_w, conv_taps, query_w, key_w, value_w, outgate_w,
         gate_w, gate_bias, mem_gain, conv_out_w, mem_out_w):
    model = key_w.shape[0]
    count = lax.axis_size(SP)
    groups = lax.axis_size(TP)
    rows = 2 * HD // count
    vmem, hbm = pl.BlockSpec(memory_space=pltpu.VMEM), pl.BlockSpec(memory_space=pltpu.HBM)
    room = lambda *arrays: [pltpu.VMEM(a.shape, a.dtype) for a in arrays]
    sems = lambda n: [pltpu.SemaphoreType.DMA((n,))]
    room = lambda *arrays: [pltpu.VMEM(a.shape, a.dtype) for a in arrays]
    sems = lambda *ns: [pltpu.SemaphoreType.DMA((n,)) for n in ns]
    small = (gate_w.reshape(model, 2).T, gate_bias.reshape(1, 2), conv_taps, key_w, value_w)
    local, gate_wt, biases, taps, key_v, value_v = call(
        prepare,
        [((1, N + 16, tokens.shape[1]), BF, V)] + [(a.shape, a.dtype, V) for a in small],
        tokens, norm_gain, *small, places=[H] * 7,
        scratch=room(tokens, norm_gain) + sems(2, 3 + 2 * CHUNKS),
    )
    tok = lax.all_gather(local, TP, axis=0, tiled=True)
    message, kv, aux = call(
        states,
        [((count, rows + 4, N), BF, A), ((N, 2 * HD), BF, A), ((8, N), F32, V)],
        tok, gate_wt, biases, key_v, value_v, flops=10**9, places=[V] * 5,
        scratch=[pltpu.VMEM((count, rows + 4, N), F32)],
    )
    arrived = exchange(message, SP, FIRST % count)
    gate_b, mixed, edge = call(
        mixing, [((N, N), BF, V), ((N, N), BF, V), ((16, N), BF, V)], tok, aux, conv_b_w, conv_c_w,
        conv_u_w, flops=10**9, places=[V] * 5, limit=16,
    )
    halo = lax.ppermute(edge, SP, [(i, i + 1) for i in range(count - 1)])
    (pack,) = call(
        inside, [((N, 3 * HD + N), F32, A)], tok, aux, kv, query_w, outgate_w, mem_gain, flops=10**9,
        places=[V, V, A, H, H, A], scratch=room(query_w, outgate_w) + sems(2 * CHUNKS),
    )
    core = lax.axis_index(TP).reshape(1).astype(jnp.int32)
    keep, send = call(
        convolve, [((N, model // 2), BF, V), ((N, model // 2), BF, V)],
        core, halo, mixed, gate_b, taps, conv_out_w,
        flops=10**9, places=[S] + [V] * 5, limit=16,
    )
    other = lax.ppermute(send, TP, [(i, i ^ 1) for i in range(groups)])
    place = lax.axis_index(SP).reshape(1).astype(jnp.int32)
    back, own = call(
        carry,
        [((count, rows, N), BF, V), ((8, N), F32, V)],
        place, arrived, flops=10**9, places=[S, V], limit=16,
        scratch=[pltpu.VMEM((count, rows + 4, N), F32), pltpu.VMEM((count, rows, N), F32)],
    )
    state = exchange(back, SP, FIRST % count)
    (mem,) = call(
        finish, [((groups, N // groups, 3 * model // 2 + N), BF, V)], state, own, pack, keep, other, mem_out_w,
        flops=10**9, scratch=[pltpu.VMEM((count, rows, N), F32)], places=[V] * 6, limit=16,
    )
    mem = exchange(mem, TP, TP_FIRST)
    (out,) = call(gather_up, [((N // groups, model), BF, A)], mem, places=[V], limit=16)
    return out


def solution(mesh):
    sp = mesh.shape["sp"]
    finer = Mesh(mesh.devices.reshape(sp, mesh.shape["tp"]), ("sp", "tp"))
    cols = P(None, TP)
    in_specs = (
        P(SP, TP), cols, cols, cols, cols, cols, cols, cols, cols, cols,
        P(None, None, TP), cols, P(TP), P(TP, None), P(TP, None),
    )
    return jax.shard_map(body, mesh=finer, in_specs=in_specs, out_specs=P((SP, TP), None), check_vma=False)
```
